32 devices in a mesh: sp: 16 (over z, y, x), tp: 2 (over core).
Axes of the slice: x: 2, y: 2, z: 4, core: 2. Of those that a mesh axis runs over, the one named last changes fastest.
Arguments:
- tokens_in: bfloat16 [2048, 2048], P(('sp', 'tp')), may hold values from -9 to 9, as said below
- w_query: bfloat16 [2048, 2048], P(None, 'tp'), may hold values from -0.125 to 0.125
- w_key: bfloat16 [2048, 512], P(None, 'tp'), may hold values from -0.125 to 0.125
- w_value: bfloat16 [2048, 512], P(None, 'tp'), may hold values from -0.125 to 0.125
- w_out: bfloat16 [2048, 2048], P('tp'), may hold values from -0.125 to 0.125
- q_gain: float32 [64], replicated, may hold values from 0.1 to 14
- k_gain: float32 [64], replicated, may hold values from 0.1 to 14
Outputs:
- attended: bfloat16 [2048, 2048], P(('sp', 'tp'))
The draws below stay inside these ranges and needn't reach their ends.
Inputs may be any that keep to these rules, and one draw needn't show every extreme that they name: `tokens_in`: activations whose mean differs from one block of 128 tokens to another.
All inputs are finite; a program needn't handle non-finite values.
Results may differ from the reference program's by a relative error of at most 0.014.
The reference program's roundings to bfloat16 on the way (of `weights` and `mixed`) count: a program that leaves them out, or rounds other values in their place, can miss the bound.
Values may be sent and summed in bfloat16 or wider, within the bound.
A program may use at most 64 MiB of HBM per device.

```python
import math
import jax
import jax.numpy as jnp
from jax import lax

D = 2048
HEADS = 32
KV_HEADS = 8
HD = 64
GRID_W = 64
TOK_DEV = 128
TOKENS = 2048
N_TP = 2


def draw_tokens_in(key, part):
    noise_key = jax.random.fold_in(key, 11)
    shift_key = jax.random.fold_in(key, 12)
    dir_key = jax.random.fold_in(key, 13)
    noise = jnp.clip(jax.random.normal(noise_key, (TOKENS, D), jnp.float32), -4.0, 4.0)
    shifts = jax.random.uniform(shift_key, (TOKENS // TOK_DEV, 1), jnp.float32, -1.5, 1.5)
    direction = jnp.clip(jax.random.normal(dir_key, (1, D), jnp.float32), -3.0, 3.0)
    offsets = jnp.repeat(shifts, TOK_DEV, axis=0) * direction
    return (noise + offsets).astype(jnp.bfloat16)


def gain_draw(key):
    return 1.0 + 0.18 * jnp.clip(jax.random.normal(key, (HD,), jnp.float32), -4.0, 4.0)


def draw_q_gain(key, part):
    return gain_draw(jax.random.fold_in(key, 21))


def draw_k_gain(key, part):
    return gain_draw(jax.random.fold_in(key, 22))


def block_levels(own_key, shape, pieces, least, top_value):
    def one(dim, blocks):
        steps = jax.random.uniform(jax.random.fold_in(jax.random.fold_in(own_key, 6), dim), (blocks,), jnp.float32, least / len(pieces), top_value / len(pieces))
        return jnp.repeat(jnp.exp(steps), shape[dim] // blocks).reshape((-1,) + (1,) * (len(shape) - dim - 1))

    level = one(*pieces[0])
    for cut in pieces[1:]:
        level = level * one(*cut)
    return level


def gaussian(rng, dims, scale, bound, cuts=(), kind=jnp.bfloat16):
    values = jax.random.normal(rng, dims, jnp.float32) * scale
    if len(cuts) > 0:
        values = block_levels(rng, dims, cuts, -0.22, 0.18) * values
    return jnp.clip(values, min=-bound, max=bound).astype(kind)


def setup_inputs(seed: int = 0) -> dict:
    key_of = jax.random.split(jax.random.key(seed), 8)
    tokens_in = draw_tokens_in(jax.random.fold_in(key_of[7], 71), 0)
    w_query = gaussian(key_of[1], (D, HEADS * HD), D ** -0.5, 0.125, ((1, 2),))
    w_key = gaussian(key_of[2], (D, KV_HEADS * HD), D ** -0.5, 0.125, ((1, 2),))
    w_value = gaussian(key_of[3], (D, KV_HEADS * HD), D ** -0.5, 0.125, ((1, 2),))
    w_out = gaussian(key_of[4], (HEADS * HD, D), (HEADS * HD) ** -0.5, 0.125, ((0, 2),))
    q_gain = draw_q_gain(jax.random.fold_in(key_of[7], 71), 0)
    k_gain = draw_k_gain(jax.random.fold_in(key_of[7], 71), 0)
    return {"tokens_in": tokens_in, "w_query": w_query, "w_key": w_key, "w_value": w_value, "w_out": w_out, "q_gain": q_gain, "k_gain": k_gain}


def turned(vectors, position, gain):
    pairs = vectors.shape[-1] // 4
    scaled = vectors * lax.rsqrt(lax.optimization_barrier(jnp.mean(vectors * vectors, axis=-1, keepdims=True)) + 1e-06) * gain
    freq = 10000.0 ** (-jnp.arange(pairs, dtype=jnp.float32) / pairs)
    grid_row = (position // GRID_W).astype(jnp.float32)
    grid_col = (position % GRID_W).astype(jnp.float32)
    angle = jnp.stack([grid_row[:, None] * freq, grid_col[:, None] * freq], axis=1)
    cosine = jnp.cos(angle)[:, None]
    sine = jnp.sin(angle)[:, None]
    split = scaled.reshape(scaled.shape[:-1] + (2, 2, pairs))
    first = split[..., 0, :]
    second = split[..., 1, :]
    joined = jnp.stack([first * cosine - second * sine, first * sine + second * cosine], axis=-2)
    return joined.reshape(scaled.shape)

def reference(tokens_in, w_query, w_key, w_value, w_out, q_gain, k_gain):
    head_dim = q_gain.shape[0]
    query = jnp.dot(tokens_in, w_query, preferred_element_type=jnp.float32).astype(jnp.bfloat16)
    key = jnp.dot(tokens_in, w_key, preferred_element_type=jnp.float32).astype(jnp.bfloat16)
    value = jnp.dot(tokens_in, w_value, preferred_element_type=jnp.float32).astype(jnp.bfloat16)
    position = jnp.arange(TOKENS, dtype=jnp.int32)
    group = HEADS // KV_HEADS
    query_n = turned(query.astype(jnp.float32).reshape(TOKENS, HEADS, head_dim), position, q_gain).astype(jnp.bfloat16)
    key_n = turned(key.astype(jnp.float32).reshape(TOKENS, KV_HEADS, head_dim), position, k_gain).astype(jnp.bfloat16)
    value_h = value.reshape(TOKENS, KV_HEADS, head_dim)
    block = math.gcd(TOKENS, 512)
    query_g = query_n.reshape(TOKENS // block, block, KV_HEADS, group, head_dim).transpose(2, 0, 3, 1, 4)
    keys_h = key_n.transpose(1, 0, 2)
    values_h = value_h.transpose(1, 0, 2)

    def one_head(packed):
        queries, keys, values = packed
        keys_f = keys.astype(jnp.float32)
        values_f = values.astype(jnp.float32)

        def one_block(qblock):
            scores = jnp.einsum('gqd,kd->gqk', qblock.astype(jnp.float32), keys_f) * head_dim ** (-0.5)
            peak = lax.optimization_barrier(jnp.max(scores, axis=-1, keepdims=True))
            expo = jnp.exp(scores - peak)
            total = lax.optimization_barrier(jnp.sum(expo, axis=-1, keepdims=True))
            weights = expo.astype(jnp.bfloat16).astype(jnp.float32)
            return (jnp.einsum('gqk,kd->gqd', weights, values_f) / total).astype(jnp.bfloat16)
        return lax.map(one_block, queries)
    mixed = lax.map(one_head, (query_g, keys_h, values_h))
    mixed = mixed.transpose(1, 3, 0, 2, 4).reshape(TOKENS, HEADS * head_dim)
    width = HEADS * head_dim // N_TP
    summed = jnp.zeros((TOKENS, w_out.shape[1]), jnp.float32)
    for index in range(N_TP):
        partial_value = jnp.dot(mixed[:, index * width:(index + 1) * width], w_out[index * width:(index + 1) * width], preferred_element_type=jnp.float32).astype(jnp.bfloat16)
        partial_value = lax.optimization_barrier(partial_value)
        summed = summed + partial_value.astype(jnp.float32)
    return summed.astype(jnp.bfloat16)
```

```python
import functools

import jax
import jax.numpy as jnp
import numpy as np
from jax import lax
from jax.experimental import pallas as pl
from jax.experimental.pallas import tpu as pltpu
from jax.sharding import PartitionSpec as P

GRID_W = 64
LANES = 128
ONES = 16
X_CUTS = 4
O_CUTS = 4
STRAIGHT = (1, 2)


def tables(token_count, head_dim):
    pairs = head_dim // 4
    lane = np.arange(LANES)
    freq = 10000.0 ** (-(lane % pairs) / pairs)
    sign = np.where(lane % (2 * pairs) < pairs, -1.0, 1.0)

    def both(count):
        angle = np.arange(count)[:, None] * freq[None, :]
        return np.concatenate([np.cos(angle), np.sin(angle) * sign], axis=1).astype(np.float32)

    return both(token_count // GRID_W), both(GRID_W)


def kernel(
    n_sp, n_tp, members, head_dim,
    tok_hbm, wq_hbm, wkv_hbms, wo_hbm, row_hbm, col_hbm, qg_hbm, kg_hbm, out_ref,
    x, wq, wkvs, wo, row_ref, col_ref, qg_ref, kg_ref,
    kv_out, kv_all, q_out, q_all, qs, vt, sc, pb, acc, peak, m_out, m_all, o_acc, o_out, o_in,
    load_sem, x_send, x_recv, kv_send, kv_recv, up_send, down_send, cross_send, on_send,
    q_send, q_recv, m_send, m_recv, o_send, o_recv,
):
    bf, f32 = jnp.bfloat16, jnp.float32
    sp, tp = lax.axis_index("sp"), lax.axis_index("tp")
    own_rows, depth = tok_hbm.shape
    rows = own_rows * n_tp
    groups = n_sp // members
    plane, member = sp // members, sp % members
    width = wq.shape[1] // members
    heads = width // head_dim
    tall = heads * rows
    keys = members * rows
    first = plane * members
    below, above = plane, groups - 1 - plane
    both_sides = jnp.minimum(below, above)

    def peer(step):
        other, bit = member, 1
        while bit <= step:
            if step & bit:
                other = other + bit - 2 * bit * ((member // bit) % 2)
            bit *= 2
        return other

    def sp_copy(src, dst, send, recv, to):
        return pltpu.make_async_remote_copy(
            src_ref=src, dst_ref=dst, send_sem=send, recv_sem=recv,
            device_id={"sp": to}, device_id_type=pl.DeviceIdType.MESH)

    def tp_copy(src, dst, send, recv, to):
        return pltpu.make_async_remote_copy(
            src_ref=src, dst_ref=dst, send_sem=send, recv_sem=recv,
            device_id={"tp": to}, device_id_type=pl.DeviceIdType.MESH)

    def own_slice(index):
        return pl.ds(pl.multiple_of(index * own_rows, own_rows), own_rows)

    def way(i):
        paired = i <= 2 * both_sides
        distance = jnp.where(paired, (i + 1) // 2, i - both_sides)
        upward = jnp.where(paired, i % 2, jnp.where(above > below, 1, 0))
        return distance, 2 * upward - 1

    barrier = pltpu.get_barrier_semaphore()
    for step in range(1, n_tp):
        pl.semaphore_signal(barrier, inc=1, device_id={"tp": (tp + step) % n_tp}, device_id_type=pl.DeviceIdType.MESH)
    for step in range(1, members):
        pl.semaphore_signal(barrier, inc=1, device_id={"sp": first + peer(step)}, device_id_type=pl.DeviceIdType.MESH)

    def greet(when, to):
        @pl.when(when)
        def _():
            pl.semaphore_signal(barrier, inc=1, device_id={"sp": to}, device_id_type=pl.DeviceIdType.MESH)

    crossing = [step for step in STRAIGHT if step < members]
    greet(below > 0, sp - members)
    greet(above > 0, sp + members)
    greet((below > 1) & (above > 0), sp - 2 * members)
    greet((above > 1) & (below > 0), sp + 2 * members)
    for step in crossing:
        greet((plane < 2) & (above > 0), (plane + 1) * members + peer(step))
        greet((plane > 0) & (above > 1), (plane + 2) * members + peer(step))

    def count(fact):
        return jnp.where(fact, 1, 0)

    targets = (n_tp - 1 + members - 1 + count(below > 0) + count(above > 0) + count(below > 2) + count(above > 2)
               + len(crossing) * count(below > 0))

    small = 1 + len(wkvs)
    pairs_of = [(tok_hbm, x.at[own_slice(tp)]), *zip(wkv_hbms, wkvs), (row_hbm, row_ref), (col_hbm, col_ref),
                (qg_hbm, qg_ref), (kg_hbm, kg_ref), (wq_hbm, wq), (wo_hbm, wo)]
    loads = [pltpu.make_async_copy(src, dst, load_sem.at[i]) for i, (src, dst) in enumerate(pairs_of)]
    for load in loads[:small + 4]:
        load.start()

    lane = lax.broadcasted_iota(jnp.int32, (rows, LANES), 1)
    low = lane % head_dim < head_dim // 2
    left = lane % (head_dim // 2) < head_dim // 4
    even = lane < head_dim
    ones_r = lax.broadcasted_iota(jnp.int32, (LANES, LANES), 0) // head_dim
    ones_c = lax.broadcasted_iota(jnp.int32, (LANES, LANES), 1) // head_dim
    block = jnp.where(ones_r == ones_c, 1.0, 0.0).astype(bf)
    vt[:ONES, :] = jnp.ones((ONES, 2 * keys), bf)

    pl.semaphore_wait(barrier, targets)
    cut_depth = depth // X_CUTS

    def x_copy(step, j):
        cols = pl.ds(j * cut_depth, cut_depth)
        return tp_copy(tok_hbm.at[:, cols], x.at[own_slice(tp), cols], x_send.at[step, j], x_recv.at[step, j],
                       (tp + step) % n_tp)

    for j in range(X_CUTS):
        for step in range(1, n_tp):
            x_copy(step, j).start()
    for load in loads[small + 4:]:
        load.start()

    for load in loads[small:small + 4]:
        load.wait()
    cos_parts, sin_parts = [], []
    per_dev = rows // GRID_W
    low_g = low[:GRID_W]
    for i in range(per_dev):
        line = row_ref[pl.ds(sp * per_dev + i, 1), :]
        cos_parts.append(jnp.where(low_g, jnp.broadcast_to(line[:, :LANES], (GRID_W, LANES)), col_ref[:, :LANES]))
        sin_parts.append(jnp.where(low_g, jnp.broadcast_to(line[:, LANES:], (GRID_W, LANES)), col_ref[:, LANES:]))
    cosine = jnp.concatenate(cos_parts, axis=0)
    sine = jnp.concatenate(sin_parts, axis=0)
    gain_q = jnp.concatenate([qg_ref[...]] * (LANES // head_dim), axis=1) * head_dim ** (-0.5)
    gain_k = jnp.concatenate([kg_ref[...]] * (LANES // head_dim), axis=1)

    def turned(u, gain):
        square = u * u
        high = square.astype(bf)
        rest = (square - high.astype(f32)).astype(bf)
        total = jnp.dot(high, block, preferred_element_type=f32) + jnp.dot(
            rest, block, preferred_element_type=f32)
        n = u * lax.rsqrt(total * (1.0 / head_dim) + 1e-06) * gain
        quarter = head_dim // 4
        other = jnp.where(left, pltpu.roll(n, LANES - quarter, 1), pltpu.roll(n, quarter, 1))
        return n * cosine + other * sine

    for load in loads[:small]:
        load.wait()
    sums = [None] * len(wkvs)
    for j in range(X_CUTS):
        cols = slice(j * cut_depth, (j + 1) * cut_depth)
        for step in range(1, n_tp):
            theirs = x.at[own_slice((tp + n_tp - step) % n_tp), pl.ds(j * cut_depth, cut_depth)]
            tp_copy(theirs, theirs, x_send.at[step, j], x_recv.at[step, j], (tp + step) % n_tp).wait_recv()
        for i in range(len(wkvs)):
            part = jnp.dot(x[:, cols], wkvs[i][cols, :], preferred_element_type=f32)
            sums[i] = part if j == 0 else sums[i] + part
    sums = [s.astype(bf).astype(f32) for s in sums]
    if len(wkvs) == 2:
        for pair in range(members // 2):
            cut = slice(pair * LANES, (pair + 1) * LANES)
            k, v = turned(sums[0][:, cut], gain_k), sums[1][:, cut]
            kv_out[2 * pair] = jnp.where(even, k, pltpu.roll(v, head_dim, 1)).astype(bf)
            kv_out[2 * pair + 1] = jnp.where(even, pltpu.roll(k, head_dim, 1), v).astype(bf)
    else:
        kv_out[0] = jnp.where(even, turned(sums[0], gain_k), sums[0]).astype(bf)

    def kv_copy(step):
        return sp_copy(kv_out.at[peer(step)], kv_all.at[sp], kv_send.at[step], kv_recv.at[sp], first + peer(step))

    def line(src, slot, send, to_plane):
        return sp_copy(src, kv_all.at[slot], send, kv_recv.at[slot], to_plane * members + member)

    def both_ways(src, slot, step, act):
        if step in crossing:
            beside, beyond = below > 2, below < 0
        else:
            beside, beyond = below > 0, below > 2

        @pl.when(beside)
        def _():
            act(line(src, slot, down_send.at[0, step], plane - 1))

        @pl.when(above > 0)
        def _():
            act(line(src, slot, up_send.at[0, step], plane + 1))

        @pl.when(beyond)
        def _():
            act(line(src, slot, down_send.at[1, step], plane - 2))

        @pl.when(above > 2)
        def _():
            act(line(src, slot, up_send.at[1, step], plane + 2))

    def straight(step, act):
        to_plane = jnp.where(plane > 2, plane - 2, plane - 1)

        @pl.when(plane > 0)
        def _():
            act(sp_copy(kv_out.at[peer(step)], kv_all.at[sp], cross_send.at[step], kv_recv.at[sp],
                        to_plane * members + peer(step)))

    def start(copy):
        copy.start()

    def wait_send(copy):
        copy.wait_send()

    def wait_kv(slot):
        sp_copy(kv_all.at[slot], kv_all.at[slot], kv_send.at[0], kv_recv.at[slot], sp).wait_recv()

    both_ways(kv_out.at[member], sp, 0, start)
    for step in range(1, members):
        kv_copy(step).start()
    for step in crossing:
        straight(step, start)
    kv_all[sp] = kv_out[member]

    loads[small + 4].wait()

    def q_copy(step):
        return sp_copy(q_out.at[step], q_all.at[step], q_send.at[step], q_recv.at[step], first + peer(step))

    def spread(step, q):
        for g in range(heads):
            u = q[:, (g // 2) * LANES:(g // 2 + 1) * LANES].astype(f32)
            u = u if g % 2 == 0 else pltpu.roll(u, head_dim, 1)
            qs[(step * heads + g) * rows:(step * heads + g + 1) * rows, :] = jnp.where(even, u, 0.0).astype(bf)

    def plane_relay(step):
        slot = first + peer(step)
        wait_kv(slot)
        both_ways(kv_all.at[slot], slot, step, start)

    def raw_queries(step):
        part = wq[:, pl.ds(pl.multiple_of(peer(step) * width, width), width)]
        return jnp.dot(x[...], part, preferred_element_type=f32)

    order = (*range(members - 1, 0, -1), 0)
    raw = raw_queries(order[0])
    for n, step in enumerate(order):
        u = raw.astype(bf).astype(f32)
        if n + 1 < members:
            raw = raw_queries(order[n + 1])
        for t in range(width // LANES):
            cut = slice(t * LANES, (t + 1) * LANES)
            q_out[step, :, cut] = turned(u[:, cut], gain_q).astype(bf)
    near_first = tuple(range(members))
    far_first = (*range(members - 1, 0, -1), 0)

    def onward(i):
        distance, side = way(i)
        target = plane - side
        inside = (target > 0) & (target < groups - 1)
        needed = (target >= 0) & (target < groups) & ((distance > 1) | jnp.logical_not(inside))
        return (plane + distance * side) * members, target, needed

    def relay(i, steps):
        base, to_plane, needed = onward(i)

        @pl.when(needed)
        def _():
            for step in steps:
                slot = base + peer(step)
                wait_kv(slot)
                line(kv_all.at[slot], slot, on_send.at[slot], to_plane).start()

    at_end = (below == 0) | (above == 0)

    def send_queries():
        for step in far_first[:-1]:
            q_copy(step).start()

    @pl.when(at_end)
    def _():
        send_queries()

    if groups > 1:
        relay(1, (0,))
    if groups > 3:
        relay(3, (0,))
    for step in near_first[1:]:
        plane_relay(step)
    @pl.when(jnp.logical_not(at_end))
    def _():
        send_queries()

    if groups > 1 and members > 1:
        relay(1, near_first[1:3])
    if groups > 2:
        relay(2, near_first)
    if groups > 3 and members > 1:
        relay(3, near_first[1:3])

    def prepare(slots):
        for c, slot in enumerate(slots):
            flipped = kv_all[slot].astype(f32).T
            vt[ONES:, c * rows:(c + 1) * rows] = flipped[head_dim:].astype(bf)

    def score(slots, step, bank):
        k = jnp.concatenate([kv_all[slot] for slot in slots], axis=0)
        sc[bank, :len(slots) * rows] = lax.dot_general(
            k, qs[step * tall:(step + 1) * tall, :], (((1,), (1,)), ((), ())), preferred_element_type=f32)

    def weigh(count, step, bank, fresh):
        place = slice(step * tall, (step + 1) * tall)
        s = sc[bank, :count]
        top = jnp.max(jnp.max(s.reshape(count // 8, 8, tall), axis=0), axis=0, keepdims=True)
        now = jnp.broadcast_to(top, (8, tall))
        fade = None
        if not fresh:
            before = peak[:, place]
            now = jnp.maximum(before, now)
            fade = jnp.exp(before - now)
        peak[:, place] = now
        pb[bank, :count] = jnp.exp(s - jnp.broadcast_to(now[:1], (count, tall))).astype(bf)
        return fade

    def gather(count, step, bank, fade):
        place = slice(step * tall, (step + 1) * tall)
        new = jnp.dot(vt[:, :count], pb[bank, :count], preferred_element_type=f32)
        if fade is not None:
            new = acc[:, place] * jnp.broadcast_to(fade[:1], (ONES + head_dim, tall)) + new
        acc[:, place] = new

    def sweep(slots, steps, fresh=False, done=None):
        count = len(slots) * rows
        prepare(slots)
        score(slots, steps[0], 0)
        fades = [None] * len(steps)
        for n, step in enumerate(steps):
            if n + 1 < len(steps):
                score(slots, steps[n + 1], (n + 1) % 2)
            fades[n] = weigh(count, step, n % 2, fresh)
            if n:
                gather(count, steps[n - 1], (n - 1) % 2, fades[n - 1])
                if done:
                    done(steps[n - 1])
        gather(count, steps[-1], (len(steps) - 1) % 2, fades[-1])
        if done:
            done(steps[-1])

    def m_copy(step):
        return sp_copy(m_out.at[step], m_all.at[step], m_send.at[step], m_recv.at[step], first + peer(step))

    def finish(step):
        for pair in range(heads // 2):
            halves = []
            for g in (2 * pair, 2 * pair + 1):
                piece = acc[:, (step * heads + g) * rows:(step * heads + g + 1) * rows]
                halves.append(piece[ONES:] * jnp.concatenate([1.0 / piece[:8]] * (head_dim // 8), axis=0))
            mixed = jnp.concatenate(halves, axis=0).T.astype(bf)
            (m_out if step else m_all)[step, :, pair * LANES:(pair + 1) * LANES] = mixed
        if step:
            m_copy(step).start()

    def slots_of(i):
        base, _, needed = onward(i)
        return [base + peer(step) for step in near_first], needed

    def fetch(slots, needed):
        @pl.when(jnp.logical_not(needed))
        def _():
            for slot in slots:
                wait_kv(slot)

    own = [sp if step == 0 else first + peer(step) for step in near_first]
    spread(0, q_out[0])
    sweep(own, (0,), fresh=True)
    if groups > 1 and members > 1:
        relay(1, near_first[3:])
        if groups > 3:
            relay(3, near_first[3:])
    for step in range(1, members):
        sp_copy(q_out.at[step], q_all.at[step], q_send.at[step], q_recv.at[step], first + peer(step)).wait_recv()
        spread(step, q_all[step])
    if members > 1:
        sweep(own, tuple(range(1, members)), fresh=True)

    def whole_group(i, carry):
        slots, needed = slots_of(i)
        fetch(slots, needed)
        sweep(slots, near_first)
        if groups > 4:
            @pl.when(i + 3 < groups)
            def _():
                relay(i + 3, near_first)
        return carry

    if groups > 1:
        joined = max(1, groups - 2)
        lax.fori_loop(1, joined, whole_group, 0)
        last_slots = []
        for i in range(joined, groups):
            slots, needed = slots_of(i)
            fetch(slots, needed)
            last_slots += slots
        sweep(last_slots, far_first, done=finish)
    else:
        for step in far_first:
            finish(step)

    loads[small + 5].wait()
    cut_out = wo.shape[1] // O_CUTS

    def o_copy(step, j):
        cols = pl.ds(j * cut_out, cut_out)
        return tp_copy(o_out.at[step, :, cols], o_in.at[step, :, cols], o_send.at[step, j], o_recv.at[step, j],
                       (tp + step) % n_tp)

    def mixed_share(step, j):
        share = pl.ds(pl.multiple_of(peer(step) * width, width), width)
        return jnp.dot(m_all[step], wo[share, j * cut_out:(j + 1) * cut_out], preferred_element_type=f32)

    for step in (0, *far_first[:-1]):
        if step:
            sp_copy(m_out.at[step], m_all.at[step], m_send.at[step], m_recv.at[step], first + peer(step)).wait_recv()
        term = mixed_share(step, 0)
        for j in range(O_CUTS):
            cols = slice(j * cut_out, (j + 1) * cut_out)
            total = o_acc[:, cols] + term if step else term
            if j + 1 < O_CUTS:
                term = mixed_share(step, j + 1)
            o_acc[:, cols] = total
            if step == min(1, members - 1):
                for other in range(1, n_tp):
                    o_out[other, :, cols] = o_acc[own_slice((tp + other) % n_tp), cols].astype(bf)
                    o_copy(other, j).start()
    for j in range(O_CUTS):
        cols = slice(j * cut_out, (j + 1) * cut_out)
        result = o_acc[own_slice(tp), cols].astype(bf).astype(f32)
        for other in range(1, n_tp):
            o_copy(other, j).wait_recv()
            result = result + o_in[other, :, cols].astype(f32)
        out_ref[:, cols] = result.astype(bf)

    for j in range(X_CUTS):
        for step in range(1, n_tp):
            x_copy(step, j).wait_send()
    for j in range(O_CUTS):
        for step in range(1, n_tp):
            o_copy(step, j).wait_send()
    both_ways(kv_out.at[member], sp, 0, wait_send)
    for step in range(1, members):
        kv_copy(step).wait_send()
        q_copy(step).wait_send()
        m_copy(step).wait_send()
        both_ways(kv_all.at[first + peer(step)], first + peer(step), step, wait_send)
        if step in crossing:
            straight(step, wait_send)

    def sent(i, carry):
        base, to_plane, needed = onward(i)

        @pl.when(needed)
        def _():
            for step in near_first:
                slot = base + peer(step)
                line(kv_all.at[slot], slot, on_send.at[slot], to_plane).wait_send()

        return carry

    lax.fori_loop(1, groups, sent, 0)


def solution(mesh):
    n_sp, n_tp = mesh.shape["sp"], mesh.shape["tp"]

    def body(tokens_in, w_query, w_key, w_value, w_out, q_gain, k_gain):
        head_dim = q_gain.shape[0]
        own_rows, depth = tokens_in.shape
        rows = own_rows * n_tp
        query_cols, key_cols = w_query.shape[1], w_key.shape[1]
        members = key_cols // head_dim
        width = query_cols // members
        heads = width // head_dim
        if key_cols % LANES:
            wkv = (jnp.concatenate([w_key, w_value], axis=1),)
        else:
            wkv = (w_key, w_value)
        row_table, col_table = tables(rows * n_sp, head_dim)
        bf, f32 = jnp.bfloat16, jnp.float32
        hbm = pl.BlockSpec(memory_space=pltpu.HBM)
        vmem = pl.BlockSpec(memory_space=pltpu.VMEM)
        dma = pltpu.SemaphoreType.DMA
        out_cols = w_out.shape[1]
        call = pl.pallas_call(
            functools.partial(kernel, n_sp, n_tp, members, head_dim),
            out_shape=pltpu.VMEM((own_rows, out_cols), bf),
            in_specs=[hbm, hbm, (hbm,) * len(wkv), hbm, hbm, hbm, hbm, hbm],
            out_specs=vmem,
            scratch_shapes=[
                pltpu.VMEM((rows, depth), bf),
                pltpu.VMEM(w_query.shape, bf),
                tuple(pltpu.VMEM(w.shape, bf) for w in wkv),
                pltpu.VMEM(w_out.shape, bf),
                pltpu.VMEM(row_table.shape, f32),
                pltpu.VMEM(col_table.shape, f32),
                pltpu.VMEM((1, head_dim), f32),
                pltpu.VMEM((1, head_dim), f32),
                pltpu.VMEM((members, rows, LANES), bf),
                pltpu.VMEM((n_sp, rows, LANES), bf),
                pltpu.VMEM((members, rows, width), bf),
                pltpu.VMEM((members, rows, width), bf),
                pltpu.VMEM((members * heads * rows, LANES), bf),
                pltpu.VMEM((ONES + head_dim, 2 * members * rows), bf),
                pltpu.VMEM((2, 2 * members * rows, heads * rows), f32),
                pltpu.VMEM((2, 2 * members * rows, heads * rows), bf),
                pltpu.VMEM((ONES + head_dim, members * heads * rows), f32),
                pltpu.VMEM((8, members * heads * rows), f32),
                pltpu.VMEM((members, rows, width), bf),
                pltpu.VMEM((members, rows, width), bf),
                pltpu.VMEM((rows, out_cols), f32),
                pltpu.VMEM((n_tp, own_rows, out_cols), bf),
                pltpu.VMEM((n_tp, own_rows, out_cols), bf),
                dma((9,)),
                dma((n_tp, X_CUTS)), dma((n_tp, X_CUTS)),
                dma((members,)), dma((n_sp,)), dma((2, members)), dma((2, members)), dma((members,)), dma((n_sp,)),
                dma((members,)), dma((members,)),
                dma((members,)), dma((members,)),
                dma((n_tp, O_CUTS)), dma((n_tp, O_CUTS)),
            ],
            compiler_params=pltpu.CompilerParams(
                collective_id=0, has_side_effects=True, vmem_limit_bytes=56 * 1024 * 1024),
        )
        return call(tokens_in, w_query, wkv, w_out, jnp.asarray(row_table), jnp.asarray(col_table),
                    q_gain.reshape(1, head_dim), k_gain.reshape(1, head_dim))

    return jax.shard_map(
        body,
        mesh=mesh,
        in_specs=(
            P(("sp", "tp"), None),
            P(None, "tp"),
            P(None, "tp"),
            P(None, "tp"),
            P("tp", None),
            P(),
            P(),
        ),
        out_specs=P(("sp", "tp"), None),
        check_vma=False,
    )
```

```python
import functools

import jax
import jax.numpy as jnp
import numpy as np
from jax import lax
from jax.experimental import pallas as pl
from jax.experimental.pallas import tpu as pltpu
from jax.sharding import PartitionSpec as P

GRID_W = 64
LANES = 128
ONES = 16
X_CUTS = 1
O_CUTS = 2
STRAIGHT = (1, 2)
LATE_BESIDE = False


def tables(token_count, head_dim):
    pairs = head_dim // 4
    lane = np.arange(LANES)
    freq = 10000.0 ** (-(lane % pairs) / pairs)
    sign = np.where(lane % (2 * pairs) < pairs, -1.0, 1.0)

    def both(count):
        angle = np.arange(count)[:, None] * freq[None, :]
        return np.concatenate([np.cos(angle), np.sin(angle) * sign], axis=1).astype(np.float32)

    return both(token_count // GRID_W), both(GRID_W)


def kernel(
    n_sp, n_tp, members, head_dim,
    tok_hbm, wq_hbm, wkv_hbms, wo_hbm, row_hbm, col_hbm, qg_hbm, kg_hbm, out_ref,
    x, wq, wkvs, wo, row_ref, col_ref, qg_ref, kg_ref,
    kv_out, kv_all, q_out, q_all, qs, vt, sc, pb, acc, peak, m_out, m_all, o_acc, o_out, o_in,
    load_sem, x_send, x_recv, kv_recv, own_send, on_send, q_recv, m_recv, o_recv,
):
    bf, f32 = jnp.bfloat16, jnp.float32
    sp, tp = lax.axis_index("sp"), lax.axis_index("tp")
    own_rows, depth = tok_hbm.shape
    rows = own_rows * n_tp
    groups = n_sp // members
    plane, member = sp // members, sp % members
    width = wq.shape[1] // members
    heads = width // head_dim
    tall = heads * rows
    keys = members * rows
    first = plane * members
    below, above = plane, groups - 1 - plane
    peers = max(1, members - 1)
    both_sides = jnp.minimum(below, above)

    def peer(step):
        other, bit = member, 1
        while bit <= step:
            if step & bit:
                other = other + bit - 2 * bit * ((member // bit) % 2)
            bit *= 2
        return other

    def sp_copy(src, dst, send, recv, to):
        return pltpu.make_async_remote_copy(
            src_ref=src, dst_ref=dst, send_sem=send, recv_sem=recv,
            device_id={"sp": to}, device_id_type=pl.DeviceIdType.MESH)

    def tp_copy(src, dst, send, recv, to):
        return pltpu.make_async_remote_copy(
            src_ref=src, dst_ref=dst, send_sem=send, recv_sem=recv,
            device_id={"tp": to}, device_id_type=pl.DeviceIdType.MESH)

    def own_slice(index):
        return pl.ds(pl.multiple_of(index * own_rows, own_rows), own_rows)

    def way(i):
        paired = i <= 2 * both_sides
        distance = jnp.where(paired, (i + 1) // 2, i - both_sides)
        upward = jnp.where(paired, i % 2, jnp.where(above > below, 1, 0))
        return distance, 2 * upward - 1

    barrier = pltpu.get_barrier_semaphore()
    for step in range(1, n_tp):
        pl.semaphore_signal(barrier, inc=1, device_id={"tp": (tp + step) % n_tp}, device_id_type=pl.DeviceIdType.MESH)
    for step in range(1, members):
        pl.semaphore_signal(barrier, inc=1, device_id={"sp": first + peer(step)}, device_id_type=pl.DeviceIdType.MESH)

    def greet(when, to):
        @pl.when(when)
        def _():
            pl.semaphore_signal(barrier, inc=1, device_id={"sp": to}, device_id_type=pl.DeviceIdType.MESH)

    crossing = [step for step in STRAIGHT if step < members]
    greet(below > 0, sp - members)
    greet(above > 0, sp + members)
    greet((below > 1) & (above > 0), sp - 2 * members)
    greet((above > 1) & (below > 0), sp + 2 * members)
    for step in crossing:
        greet((plane < 2) & (above > 0), (plane + 1) * members + peer(step))
        greet((plane > 1) & (above > 1), (plane + 2) * members + peer(step))
        greet((plane == 0) & (above > 2), (plane + 3) * members + peer(step))
    greet((plane == 0) & (above > 2), sp + 3 * members)

    def count(fact):
        return jnp.where(fact, 1, 0)

    targets = (n_tp - 1 + members - 1 + count(below > 0) + count(above > 0) + count(below > 2) + count(above > 2) + count(below == 3)
               + len(crossing) * count(below > 0))

    small = 1 + len(wkvs)
    pairs_of = [(tok_hbm, x.at[own_slice(tp)]), *zip(wkv_hbms, wkvs), (row_hbm, row_ref), (col_hbm, col_ref),
                (qg_hbm, qg_ref), (kg_hbm, kg_ref), (wq_hbm, wq), (wo_hbm, wo)]
    loads = [pltpu.make_async_copy(src, dst, load_sem.at[(i + 1) % len(pairs_of)]) for i, (src, dst) in enumerate(pairs_of)]
    for load in loads:
        load.start()

    lane = lax.broadcasted_iota(jnp.int32, (rows, LANES), 1)
    low = lane % head_dim < head_dim // 2
    left = lane % (head_dim // 2) < head_dim // 4
    even = lane < head_dim
    ones_r = lax.broadcasted_iota(jnp.int32, (LANES, LANES), 0) // head_dim
    ones_c = lax.broadcasted_iota(jnp.int32, (LANES, LANES), 1) // head_dim
    block = jnp.where(ones_r == ones_c, 1.0, 0.0).astype(bf)
    vt[:ONES, :] = jnp.ones((ONES, 3 * keys), bf)

    loads[0].wait()
    pl.semaphore_wait(barrier, targets)
    cut_depth = depth // X_CUTS

    def x_copy(step, j):
        cols = pl.ds(j * cut_depth, cut_depth)
        return tp_copy(x.at[own_slice(tp), cols], x.at[own_slice(tp), cols], x_send.at[step - 1, j], x_recv.at[step - 1, j],
                       (tp + step) % n_tp)

    for j in range(X_CUTS):
        for step in range(1, n_tp):
            x_copy(step, j).start()
    for load in loads[small:small + 4]:
        load.wait()
    cos_parts, sin_parts = [], []
    per_dev = rows // GRID_W
    low_g = low[:GRID_W]
    for i in range(per_dev):
        line = row_ref[pl.ds(sp * per_dev + i, 1), :]
        cos_parts.append(jnp.where(low_g, jnp.broadcast_to(line[:, :LANES], (GRID_W, LANES)), col_ref[:, :LANES]))
        sin_parts.append(jnp.where(low_g, jnp.broadcast_to(line[:, LANES:], (GRID_W, LANES)), col_ref[:, LANES:]))
    cosine = jnp.concatenate(cos_parts, axis=0)
    sine = jnp.concatenate(sin_parts, axis=0)
    gain_q = jnp.concatenate([qg_ref[...]] * (LANES // head_dim), axis=1) * head_dim ** (-0.5)
    gain_k = jnp.concatenate([kg_ref[...]] * (LANES // head_dim), axis=1)

    def turned(u, gain):
        square = u * u
        high = square.astype(bf)
        rest = (square - high.astype(f32)).astype(bf)
        total = jnp.dot(high, block, preferred_element_type=f32) + jnp.dot(
            rest, block, preferred_element_type=f32)
        n = u * lax.rsqrt(total * (1.0 / head_dim) + 1e-06) * gain
        quarter = head_dim // 4
        other = jnp.where(left, pltpu.roll(n, LANES - quarter, 1), pltpu.roll(n, quarter, 1))
        return n * cosine + other * sine

    for load in loads[1:small]:
        load.wait()
    sums = [None] * len(wkvs)
    for j in range(X_CUTS):
        cols = slice(j * cut_depth, (j + 1) * cut_depth)
        for step in range(1, n_tp):
            theirs = x.at[own_slice((tp + n_tp - step) % n_tp), pl.ds(j * cut_depth, cut_depth)]
            tp_copy(theirs, theirs, x_send.at[step - 1, j], x_recv.at[step - 1, j], (tp + step) % n_tp).wait_recv()
        for i in range(len(wkvs)):
            part = jnp.dot(x[:, cols], wkvs[i][cols, :], preferred_element_type=f32)
            sums[i] = part if j == 0 else sums[i] + part
    sums = [s.astype(bf).astype(f32) for s in sums]
    if len(wkvs) == 2:
        for pair in range(members // 2):
            cut = slice(pair * LANES, (pair + 1) * LANES)
            k, v = turned(sums[0][:, cut], gain_k), sums[1][:, cut]
            kv_out[2 * pair] = jnp.where(even, k, pltpu.roll(v, head_dim, 1)).astype(bf)
            kv_out[2 * pair + 1] = jnp.where(even, pltpu.roll(k, head_dim, 1), v).astype(bf)
    else:
        kv_out[0] = jnp.where(even, turned(sums[0], gain_k), sums[0]).astype(bf)

    def kv_copy(step):
        return sp_copy(kv_out.at[peer(step)], kv_all.at[sp], load_sem.at[step], kv_recv.at[sp], first + peer(step))

    def line(src, slot, send, to_plane):
        return sp_copy(src, kv_all.at[slot], send, kv_recv.at[slot], to_plane * members + member)

    def both_ways(src, slot, step, act, late=False):
        if step in crossing:
            far, beside, beyond = below < 0, below > 2, below == 3
        else:
            far, beside, beyond = below == 3, below > 0, below > 2
        if late:
            @pl.when(below == 3)
            def _():
                if LATE_BESIDE:
                    act(line(src, slot, own_send.at[0, step], plane - 1))
                act(line(src, slot, own_send.at[own_send.shape[0] - 1 if groups > 4 else 1, step], plane - 2))

            return

        @pl.when(far)
        def _():
            act(line(src, slot, own_send.at[2, step], plane - 3))

        @pl.when(beside & (below != 3) if LATE_BESIDE else beside)
        def _():
            act(line(src, slot, own_send.at[0, step], plane - 1))

        @pl.when(above > 0)
        def _():
            act(line(src, slot, own_send.at[1, step], plane + 1))

        @pl.when(beyond & (below != 3))
        def _():
            act(line(src, slot, own_send.at[own_send.shape[0] - 1 if groups > 4 else 1, step], plane - 2))

        @pl.when(above > 2)
        def _():
            act(line(src, slot, own_send.at[2, step], plane + 2))

    def straight(step, act):
        to_plane = jnp.where(plane > 3, plane - 2, jnp.where(plane == 3, plane - 3, plane - 1))

        @pl.when(plane > 0)
        def _():
            act(sp_copy(kv_out.at[peer(step)], kv_all.at[sp], own_send.at[jnp.where(plane > 3, own_send.shape[0] - 1, jnp.where(plane == 3, 2, 0)), step], kv_recv.at[sp],
                        to_plane * members + peer(step)))

    def start(copy):
        copy.start()

    def wait_send(copy):
        copy.wait_send()

    def wait_kv(slot):
        sp_copy(kv_all.at[slot], kv_all.at[slot], load_sem.at[1], kv_recv.at[slot], sp).wait_recv()

    both_ways(kv_out.at[member], sp, 0, start)
    for step in range(1, members):
        kv_copy(step).start()
    for step in crossing:
        straight(step, start)
    kv_all[sp] = kv_out[member]

    loads[small + 4].wait()

    def q_copy(step):
        return sp_copy(q_out.at[step], q_all.at[step], load_sem.at[peers + step], q_recv.at[step - 1], first + peer(step))

    def spread(step, q):
        for g in range(heads):
            u = q[:, (g // 2) * LANES:(g // 2 + 1) * LANES].astype(f32)
            u = u if g % 2 == 0 else pltpu.roll(u, head_dim, 1)
            qs[(step * heads + g) * rows:(step * heads + g + 1) * rows, :] = jnp.where(even, u, 0.0).astype(bf)

    def plane_relay(step):
        slot = first + peer(step)
        wait_kv(slot)
        both_ways(kv_all.at[slot], slot, step, start)

    def raw_queries(step):
        part = wq[:, pl.ds(pl.multiple_of(peer(step) * width, width), width)]
        return jnp.dot(x[...], part, preferred_element_type=f32)

    order = (*range(members - 1, 0, -1), 0)
    raw = raw_queries(order[0])
    for n, step in enumerate(order):
        u = raw.astype(bf).astype(f32)
        if n + 1 < members:
            raw = raw_queries(order[n + 1])
        for t in range(width // LANES):
            cut = slice(t * LANES, (t + 1) * LANES)
            q_out[step, :, cut] = turned(u[:, cut], gain_q).astype(bf)
    near_first = tuple(range(members))
    far_first = (*range(members - 1, 0, -1), 0)

    def onward(i):
        distance, side = way(i)
        target = plane - side
        inside = (target > 0) & (target < groups - 1)
        beyond = (distance > 1) & jnp.logical_not((distance == 2) & (target == 0) & (side > 0))
        needed = (target >= 0) & (target < groups) & (beyond | ((distance == 1) & jnp.logical_not(inside)))
        return (plane + distance * side) * members, target, needed

    def relay(i, steps):
        base, to_plane, needed = onward(i)

        @pl.when(needed)
        def _():
            for step in steps:
                slot = base + peer(step)
                wait_kv(slot)
                line(kv_all.at[slot], slot, on_send.at[i if groups > 4 else i % 2, step], to_plane).start()

    at_end = (below == 0) | (above == 0)

    def send_queries():
        for step in far_first[:-1]:
            q_copy(step).start()

    @pl.when(at_end)
    def _():
        send_queries()

    if groups > 1:
        relay(1, (0,))
    if groups > 3:
        relay(3, (0,))
    for step in near_first[1:]:
        plane_relay(step)
    @pl.when(jnp.logical_not(at_end))
    def _():
        send_queries()

    def late_ways(act):
        both_ways(kv_out.at[member], sp, 0, act, late=True)
        for step in near_first[1:]:
            both_ways(kv_all.at[first + peer(step)], first + peer(step), step, act, late=True)

    late_ways(start)
    if groups > 1 and members > 1:
        relay(1, near_first[1:])
    if groups > 2:
        relay(2, (0,))

    def prepare(slots, offset):
        for c, slot in enumerate(slots):
            flipped = kv_all[slot].astype(f32).T
            vt[ONES:, offset + c * rows:offset + (c + 1) * rows] = flipped[head_dim:].astype(bf)

    def score(slots, step, bank):
        k = jnp.concatenate([kv_all[slot] for slot in slots], axis=0)
        sc[bank, :len(slots) * rows] = lax.dot_general(
            k, qs[step * tall:(step + 1) * tall, :], (((1,), (1,)), ((), ())), preferred_element_type=f32)

    def weigh(count, step, bank, fresh):
        place = slice(step * tall, (step + 1) * tall)
        s = sc[bank, :count]
        top = jnp.max(jnp.max(s.reshape(count // 8, 8, tall), axis=0), axis=0, keepdims=True)
        now = jnp.broadcast_to(top, (8, tall))
        fade = None
        if not fresh:
            before = peak[:, place]
            now = jnp.maximum(before, now)
            fade = jnp.exp(before - now)
        peak[:, place] = now
        pb[bank, :count] = jnp.exp(s - jnp.broadcast_to(now[:1], (count, tall))).astype(bf)
        return fade

    def gather(offset, count, step, bank, fade):
        place = slice(step * tall, (step + 1) * tall)
        new = jnp.dot(vt[:, offset:offset + count], pb[bank, :count], preferred_element_type=f32)
        if fade is not None:
            new = acc[:, place] * jnp.broadcast_to(fade[:1], (ONES + head_dim, tall)) + new
        acc[:, place] = new

    def run(tasks, fresh=False):
        score(tasks[0][0], tasks[0][2], 0)
        fades = []
        for n in range(len(tasks) + 1):
            if n + 1 < len(tasks):
                score(tasks[n + 1][0], tasks[n + 1][2], (n + 1) % 2)
            if n < len(tasks):
                fades.append(weigh(len(tasks[n][0]) * rows, tasks[n][2], n % 2, fresh))
            if n:
                slots, offset, step, last = tasks[n - 1]
                gather(offset, len(slots) * rows, step, (n - 1) % 2, fades[n - 1])
                if last:
                    finish(step)

    def m_copy(step):
        return sp_copy(m_out.at[step], m_all.at[step], load_sem.at[peers + step], m_recv.at[step - 1], first + peer(step))

    def finish(step):
        for pair in range(heads // 2):
            halves = []
            for g in (2 * pair, 2 * pair + 1):
                piece = acc[:, (step * heads + g) * rows:(step * heads + g + 1) * rows]
                halves.append(piece[ONES:] * jnp.concatenate([1.0 / piece[:8]] * (head_dim // 8), axis=0))
            mixed = jnp.concatenate(halves, axis=0).T.astype(bf)
            (m_out if step else m_all)[step, :, pair * LANES:(pair + 1) * LANES] = mixed
        if step:
            m_copy(step).start()

    def slots_of(i):
        base, _, needed = onward(i)
        return [base + peer(step) for step in near_first], needed

    def fetch(slots, needed):
        @pl.when(jnp.logical_not(needed))
        def _():
            for slot in slots:
                wait_kv(slot)

    own = [sp if step == 0 else first + peer(step) for step in near_first]
    spread(0, q_out[0])
    prepare(own, 0)
    run([(own, 0, 0, False)], fresh=True)
    if groups > 2 and members > 1:
        relay(2, near_first[1:])
    if groups > 3 and members > 1:
        relay(3, near_first[1:])
    for step in range(1, members):
        sp_copy(q_out.at[step], q_all.at[step], load_sem.at[peers + step], q_recv.at[step - 1], first + peer(step)).wait_recv()
        spread(step, q_all[step])
    if members > 1:
        run([(own, 0, step, False) for step in near_first[1:]], fresh=True)

    deferred = groups == 4 and members > 1
    spare = 2 * keys

    def whole_group(i, carry):
        slots, needed = slots_of(i)
        fetch(slots, needed)
        prepare(slots, spare)
        run([(slots, spare, step, False) for step in near_first[1 if deferred else 0:]])
        if groups > 4:
            @pl.when(i + 3 < groups)
            def _():
                relay(i + 3, near_first)
        return carry

    if groups > 1:
        joined = max(1, groups - 2)
        if deferred:
            whole_group(1, 0)
        else:
            lax.fori_loop(1, joined, whole_group, 0)
        last_slots = []
        for i in range(joined, groups):
            slots, needed = slots_of(i)
            fetch(slots, needed)
            prepare(slots, len(last_slots) * rows)
            last_slots += slots
        tasks = [(last_slots, 0, step, True) for step in far_first]
        if deferred:
            tasks.insert(-1, (slots_of(1)[0], spare, 0, False))
        for step in near_first[1:]:
            q_copy(step).wait_send()
        run(tasks)
    else:
        for step in near_first[1:]:
            q_copy(step).wait_send()
        for step in far_first:
            finish(step)

    loads[small + 5].wait()
    cut_out = wo.shape[1] // O_CUTS

    def o_copy(step, j):
        cols = pl.ds(j * cut_out, cut_out)
        return tp_copy(o_out.at[step, :, cols], o_in.at[step, :, cols], load_sem.at[1 + 2 * peers + (step - 1) * O_CUTS + j], o_recv.at[step - 1, j],
                       (tp + step) % n_tp)

    def mixed_share(step, j):
        share = pl.ds(pl.multiple_of(peer(step) * width, width), width)
        return jnp.dot(m_all[step], wo[share, j * cut_out:(j + 1) * cut_out], preferred_element_type=f32)

    for step in (0, *far_first[:-1]):
        if step:
            sp_copy(m_out.at[step], m_all.at[step], load_sem.at[peers + step], m_recv.at[step - 1], first + peer(step)).wait_recv()
        term = mixed_share(step, 0)
        for j in range(O_CUTS):
            cols = slice(j * cut_out, (j + 1) * cut_out)
            total = o_acc[:, cols] + term if step else term
            if j + 1 < O_CUTS:
                term = mixed_share(step, j + 1)
            o_acc[:, cols] = total
            if step == min(1, members - 1):
                for other in range(1, n_tp):
                    o_out[other, :, cols] = o_acc[own_slice((tp + other) % n_tp), cols].astype(bf)
                    o_copy(other, j).start()
    for j in range(O_CUTS):
        cols = slice(j * cut_out, (j + 1) * cut_out)
        result = o_acc[own_slice(tp), cols].astype(bf).astype(f32)
        for other in range(1, n_tp):
            o_copy(other, j).wait_recv()
            result = result + o_in[other, :, cols].astype(f32)
        out_ref[:, cols] = result.astype(bf)

    for j in range(X_CUTS):
        for step in range(1, n_tp):
            x_copy(step, j).wait_send()
    for j in range(O_CUTS):
        for step in range(1, n_tp):
            o_copy(step, j).wait_send()
    both_ways(kv_out.at[member], sp, 0, wait_send)
    late_ways(wait_send)
    for step in range(1, members):
        kv_copy(step).wait_send()
        m_copy(step).wait_send()
        both_ways(kv_all.at[first + peer(step)], first + peer(step), step, wait_send)
        if step in crossing:
            straight(step, wait_send)

    def sent(i, carry):
        base, to_plane, needed = onward(i)

        @pl.when(needed)
        def _():
            for step in near_first:
                slot = base + peer(step)
                line(kv_all.at[slot], slot, on_send.at[i if groups > 4 else i % 2, step], to_plane).wait_send()

        return carry

    lax.fori_loop(1, groups, sent, 0)


def solution(mesh):
    n_sp, n_tp = mesh.shape["sp"], mesh.shape["tp"]

    def body(tokens_in, w_query, w_key, w_value, w_out, q_gain, k_gain):
        head_dim = q_gain.shape[0]
        own_rows, depth = tokens_in.shape
        rows = own_rows * n_tp
        query_cols, key_cols = w_query.shape[1], w_key.shape[1]
        members = key_cols // head_dim
        width = query_cols // members
        heads = width // head_dim
        if key_cols % LANES:
            wkv = (jnp.concatenate([w_key, w_value], axis=1),)
        else:
            wkv = (w_key, w_value)
        row_table, col_table = tables(rows * n_sp, head_dim)
        bf, f32 = jnp.bfloat16, jnp.float32
        hbm = pl.BlockSpec(memory_space=pltpu.HBM)
        vmem = pl.BlockSpec(memory_space=pltpu.VMEM)
        dma = pltpu.SemaphoreType.DMA
        out_cols = w_out.shape[1]
        groups, peers = n_sp // members, max(1, members - 1)
        call = pl.pallas_call(
            functools.partial(kernel, n_sp, n_tp, members, head_dim),
            out_shape=pltpu.VMEM((own_rows, out_cols), bf),
            in_specs=[hbm, hbm, (hbm,) * len(wkv), hbm, hbm, hbm, hbm, hbm],
            out_specs=vmem,
            scratch_shapes=[
                pltpu.VMEM((rows, depth), bf),
                pltpu.VMEM(w_query.shape, bf),
                tuple(pltpu.VMEM(w.shape, bf) for w in wkv),
                pltpu.VMEM(w_out.shape, bf),
                pltpu.VMEM(row_table.shape, f32),
                pltpu.VMEM(col_table.shape, f32),
                pltpu.VMEM((1, head_dim), f32),
                pltpu.VMEM((1, head_dim), f32),
                pltpu.VMEM((members, rows, LANES), bf),
                pltpu.VMEM((n_sp, rows, LANES), bf),
                pltpu.VMEM((members, rows, width), bf),
                pltpu.VMEM((members, rows, width), bf),
                pltpu.VMEM((members * heads * rows, LANES), bf),
                pltpu.VMEM((ONES + head_dim, 3 * members * rows), bf),
                pltpu.VMEM((2, 2 * members * rows, heads * rows), f32),
                pltpu.VMEM((2, 2 * members * rows, heads * rows), bf),
                pltpu.VMEM((ONES + head_dim, members * heads * rows), f32),
                pltpu.VMEM((8, members * heads * rows), f32),
                pltpu.VMEM((members, rows, width), bf),
                pltpu.VMEM((members, rows, width), bf),
                pltpu.VMEM((rows, out_cols), f32),
                pltpu.VMEM((n_tp, own_rows, out_cols), bf),
                pltpu.VMEM((n_tp, own_rows, out_cols), bf),
                dma((max(7 + len(wkv), 1 + 2 * peers + (n_tp - 1) * O_CUTS),)),
                dma((n_tp - 1, X_CUTS)), dma((n_tp - 1, X_CUTS)),
                dma((n_sp,)), dma((3 if groups <= 4 else 4, members)),
                dma((2 if groups <= 4 else groups, members)),
                dma((peers,)), dma((peers,)),
                dma((n_tp - 1, O_CUTS)),
            ],
            compiler_params=pltpu.CompilerParams(
                collective_id=0, has_side_effects=True, vmem_limit_bytes=56 * 1024 * 1024),
        )
        return call(tokens_in, w_query, wkv, w_out, jnp.asarray(row_table), jnp.asarray(col_table),
                    q_gain.reshape(1, head_dim), k_gain.reshape(1, head_dim))

    return jax.shard_map(
        body,
        mesh=mesh,
        in_specs=(
            P(("sp", "tp"), None),
            P(None, "tp"),
            P(None, "tp"),
            P(None, "tp"),
            P("tp", None),
            P(),
            P(),
        ),
        out_specs=P(("sp", "tp"), None),
        check_vma=False,
    )
```

```python
import functools

import jax
import jax.numpy as jnp
import numpy as np
from jax import lax
from jax.experimental import pallas as pl
from jax.experimental.pallas import tpu as pltpu
from jax.sharding import PartitionSpec as P

GRID_W = 64
LANES = 128
ONES = 16
X_CUTS = 1
O_CUTS = 2
STRAIGHT = (1, 2)
HALVES = False
LATE_BESIDE = False


def tables(token_count, head_dim):
    pairs = head_dim // 4
    lane = np.arange(LANES)
    freq = 10000.0 ** (-(lane % pairs) / pairs)
    sign = np.where(lane % (2 * pairs) < pairs, -1.0, 1.0)

    def both(count):
        angle = np.arange(count)[:, None] * freq[None, :]
        return np.concatenate([np.cos(angle), np.sin(angle) * sign], axis=1).astype(np.float32)

    return both(token_count // GRID_W), both(GRID_W)


def kernel(
    n_sp, n_tp, members, head_dim,
    tok_hbm, wq_hbm, wkv_hbms, wo_hbm, row_hbm, col_hbm, qg_hbm, kg_hbm, out_ref,
    x, wq, wkvs, wo, row_ref, col_ref, qg_ref, kg_ref,
    kv_out, kv_all, q_out, q_all, qs, vt, sc, pb, acc, peak, m_out, m_all, o_acc, o_out, o_in,
    load_sem, x_send, x_recv, kv_recv, own_send, on_send, q_recv, m_recv, o_recv,
):
    bf, f32 = jnp.bfloat16, jnp.float32
    sp, tp = lax.axis_index("sp"), lax.axis_index("tp")
    own_rows, depth = tok_hbm.shape
    rows = own_rows * n_tp
    groups = n_sp // members
    plane, member = sp // members, sp % members
    width = wq.shape[1] // members
    heads = width // head_dim
    tall = heads * rows
    keys = members * rows
    first = plane * members
    below, above = plane, groups - 1 - plane
    peers = max(1, members - 1)
    both_sides = jnp.minimum(below, above)

    def peer(step):
        other, bit = member, 1
        while bit <= step:
            if step & bit:
                other = other + bit - 2 * bit * ((member // bit) % 2)
            bit *= 2
        return other

    def sp_copy(src, dst, send, recv, to):
        return pltpu.make_async_remote_copy(
            src_ref=src, dst_ref=dst, send_sem=send, recv_sem=recv,
            device_id={"sp": to}, device_id_type=pl.DeviceIdType.MESH)

    def tp_copy(src, dst, send, recv, to):
        return pltpu.make_async_remote_copy(
            src_ref=src, dst_ref=dst, send_sem=send, recv_sem=recv,
            device_id={"tp": to}, device_id_type=pl.DeviceIdType.MESH)

    def own_slice(index):
        return pl.ds(pl.multiple_of(index * own_rows, own_rows), own_rows)

    def way(i):
        paired = i <= 2 * both_sides
        distance = jnp.where(paired, (i + 1) // 2, i - both_sides)
        upward = jnp.where(paired, i % 2, jnp.where(above > below, 1, 0))
        return distance, 2 * upward - 1

    barrier = pltpu.get_barrier_semaphore()
    for step in range(1, n_tp):
        pl.semaphore_signal(barrier, inc=1, device_id={"tp": (tp + step) % n_tp}, device_id_type=pl.DeviceIdType.MESH)
    for step in range(1, members):
        pl.semaphore_signal(barrier, inc=1, device_id={"sp": first + peer(step)}, device_id_type=pl.DeviceIdType.MESH)

    def greet(when, to):
        @pl.when(when)
        def _():
            pl.semaphore_signal(barrier, inc=1, device_id={"sp": to}, device_id_type=pl.DeviceIdType.MESH)

    crossing = [step for step in STRAIGHT if step < members]
    greet(below > 0, sp - members)
    greet(above > 0, sp + members)
    greet((below > 1) & (above > 0), sp - 2 * members)
    greet((above > 1) & (below > 0), sp + 2 * members)
    for step in crossing:
        greet((plane < 2) & (above > 0), (plane + 1) * members + peer(step))
        greet((plane > 1) & (above > 1), (plane + 2) * members + peer(step))
        greet((plane == 0) & (above > 2), (plane + 3) * members + peer(step))
    greet((plane == 0) & (above > 2), sp + 3 * members)

    def count(fact):
        return jnp.where(fact, 1, 0)

    targets = (n_tp - 1 + members - 1 + count(below > 0) + count(above > 0) + count(below > 2) + count(above > 2) + count(below == 3)
               + len(crossing) * count(below > 0))

    small = 1 + len(wkvs)
    pairs_of = [(tok_hbm, x.at[own_slice(tp)]), *zip(wkv_hbms, wkvs), (row_hbm, row_ref), (col_hbm, col_ref),
                (qg_hbm, qg_ref), (kg_hbm, kg_ref), (wq_hbm, wq), (wo_hbm, wo)]
    loads = [pltpu.make_async_copy(src, dst, load_sem.at[(i + 1) % len(pairs_of)]) for i, (src, dst) in enumerate(pairs_of)]
    for load in loads:
        load.start()

    lane = lax.broadcasted_iota(jnp.int32, (rows, LANES), 1)
    low = lane % head_dim < head_dim // 2
    left = lane % (head_dim // 2) < head_dim // 4
    even = lane < head_dim
    ones_r = lax.broadcasted_iota(jnp.int32, (LANES, LANES), 0) // head_dim
    ones_c = lax.broadcasted_iota(jnp.int32, (LANES, LANES), 1) // head_dim
    block = jnp.where(ones_r == ones_c, 1.0, 0.0).astype(bf)
    vt[:ONES, :] = jnp.ones((ONES, 3 * keys), bf)

    loads[0].wait()
    pl.semaphore_wait(barrier, targets)
    cut_depth = depth // X_CUTS

    def x_copy(step, j):
        cols = pl.ds(j * cut_depth, cut_depth)
        return tp_copy(x.at[own_slice(tp), cols], x.at[own_slice(tp), cols], x_send.at[step - 1, j], x_recv.at[step - 1, j],
                       (tp + step) % n_tp)

    for j in range(X_CUTS):
        for step in range(1, n_tp):
            x_copy(step, j).start()
    for load in loads[small:small + 4]:
        load.wait()
    cos_parts, sin_parts = [], []
    per_dev = rows // GRID_W
    low_g = low[:GRID_W]
    for i in range(per_dev):
        line = row_ref[pl.ds(sp * per_dev + i, 1), :]
        cos_parts.append(jnp.where(low_g, jnp.broadcast_to(line[:, :LANES], (GRID_W, LANES)), col_ref[:, :LANES]))
        sin_parts.append(jnp.where(low_g, jnp.broadcast_to(line[:, LANES:], (GRID_W, LANES)), col_ref[:, LANES:]))
    cosine = jnp.concatenate(cos_parts, axis=0)
    sine = jnp.concatenate(sin_parts, axis=0)
    gain_q = jnp.concatenate([qg_ref[...]] * (LANES // head_dim), axis=1) * head_dim ** (-0.5)
    gain_k = jnp.concatenate([kg_ref[...]] * (LANES // head_dim), axis=1)

    def turned(u, gain):
        square = u * u
        high = square.astype(bf)
        rest = (square - high.astype(f32)).astype(bf)
        total = jnp.dot(high, block, preferred_element_type=f32) + jnp.dot(
            rest, block, preferred_element_type=f32)
        n = u * lax.rsqrt(total * (1.0 / head_dim) + 1e-06) * gain
        quarter = head_dim // 4
        other = jnp.where(left, pltpu.roll(n, LANES - quarter, 1), pltpu.roll(n, quarter, 1))
        return n * cosine + other * sine

    for load in loads[1:small]:
        load.wait()
    sums = [None] * len(wkvs)
    for j in range(X_CUTS):
        cols = slice(j * cut_depth, (j + 1) * cut_depth)
        for step in range(1, n_tp):
            theirs = x.at[own_slice((tp + n_tp - step) % n_tp), pl.ds(j * cut_depth, cut_depth)]
            tp_copy(theirs, theirs, x_send.at[step - 1, j], x_recv.at[step - 1, j], (tp + step) % n_tp).wait_recv()
        for i in range(len(wkvs)):
            part = jnp.dot(x[:, cols], wkvs[i][cols, :], preferred_element_type=f32)
            sums[i] = part if j == 0 else sums[i] + part
    sums = [s.astype(bf).astype(f32) for s in sums]
    if len(wkvs) == 2:
        for pair in range(members // 2):
            cut = slice(pair * LANES, (pair + 1) * LANES)
            k, v = turned(sums[0][:, cut], gain_k), sums[1][:, cut]
            kv_out[2 * pair] = jnp.where(even, k, pltpu.roll(v, head_dim, 1)).astype(bf)
            kv_out[2 * pair + 1] = jnp.where(even, pltpu.roll(k, head_dim, 1), v).astype(bf)
    else:
        kv_out[0] = jnp.where(even, turned(sums[0], gain_k), sums[0]).astype(bf)

    def kv_copy(step):
        return sp_copy(kv_out.at[peer(step)], kv_all.at[sp], load_sem.at[step], kv_recv.at[sp], first + peer(step))

    def line(src, slot, send, to_plane):
        return sp_copy(src, kv_all.at[slot], send, kv_recv.at[slot], to_plane * members + member)

    def both_ways(src, slot, step, act, late=False):
        if step in crossing:
            far, beside, beyond = below < 0, below > 2, below == 3
        else:
            far, beside, beyond = below == 3, below > 0, below > 2
        if late:
            @pl.when(below == 3)
            def _():
                if LATE_BESIDE:
                    act(line(src, slot, own_send.at[0, step], plane - 1))
                act(line(src, slot, own_send.at[own_send.shape[0] - 1 if groups > 4 else 1, step], plane - 2))

            return

        @pl.when(far)
        def _():
            act(line(src, slot, own_send.at[2, step], plane - 3))

        @pl.when(beside & (below != 3) if LATE_BESIDE else beside)
        def _():
            act(line(src, slot, own_send.at[0, step], plane - 1))

        @pl.when(above > 0)
        def _():
            act(line(src, slot, own_send.at[1, step], plane + 1))

        @pl.when(beyond & (below != 3))
        def _():
            act(line(src, slot, own_send.at[own_send.shape[0] - 1 if groups > 4 else 1, step], plane - 2))

        @pl.when(above > 2)
        def _():
            act(line(src, slot, own_send.at[2, step], plane + 2))

    def straight(step, act):
        to_plane = jnp.where(plane > 3, plane - 2, jnp.where(plane == 3, plane - 3, plane - 1))

        @pl.when(plane > 0)
        def _():
            act(sp_copy(kv_out.at[peer(step)], kv_all.at[sp], own_send.at[jnp.where(plane > 3, own_send.shape[0] - 1, jnp.where(plane == 3, 2, 0)), step], kv_recv.at[sp],
                        to_plane * members + peer(step)))

    def start(copy):
        copy.start()

    def wait_send(copy):
        copy.wait_send()

    def wait_kv(slot):
        sp_copy(kv_all.at[slot], kv_all.at[slot], load_sem.at[1], kv_recv.at[slot], sp).wait_recv()

    both_ways(kv_out.at[member], sp, 0, start)
    for step in range(1, members):
        kv_copy(step).start()
    for step in crossing:
        straight(step, start)
    kv_all[sp] = kv_out[member]

    loads[small + 4].wait()

    def q_copy(step):
        return sp_copy(q_out.at[step], q_all.at[step], load_sem.at[peers + step], q_recv.at[step - 1], first + peer(step))

    def spread(step, q):
        for g in range(heads):
            u = q[:, (g // 2) * LANES:(g // 2 + 1) * LANES].astype(f32)
            u = u if g % 2 == 0 else pltpu.roll(u, head_dim, 1)
            qs[(step * heads + g) * rows:(step * heads + g + 1) * rows, :] = jnp.where(even, u, 0.0).astype(bf)

    def plane_relay(step):
        slot = first + peer(step)
        wait_kv(slot)
        both_ways(kv_all.at[slot], slot, step, start)

    def raw_queries(step):
        part = wq[:, pl.ds(pl.multiple_of(peer(step) * width, width), width)]
        return jnp.dot(x[...], part, preferred_element_type=f32)

    order = (*range(members - 1, 0, -1), 0)
    raw = raw_queries(order[0])
    for n, step in enumerate(order):
        u = raw.astype(bf).astype(f32)
        if n + 1 < members:
            raw = raw_queries(order[n + 1])
        for t in range(width // LANES):
            cut = slice(t * LANES, (t + 1) * LANES)
            q_out[step, :, cut] = turned(u[:, cut], gain_q).astype(bf)
    near_first = tuple(range(members))
    far_first = (*range(members - 1, 0, -1), 0)

    def onward(i):
        distance, side = way(i)
        target = plane - side
        inside = (target > 0) & (target < groups - 1)
        beyond = (distance > 1) & jnp.logical_not((distance == 2) & (target == 0) & (side > 0))
        needed = (target >= 0) & (target < groups) & (beyond | ((distance == 1) & jnp.logical_not(inside)))
        return (plane + distance * side) * members, target, needed

    def relay(i, steps):
        base, to_plane, needed = onward(i)

        @pl.when(needed)
        def _():
            for step in steps:
                slot = base + peer(step)
                wait_kv(slot)
                line(kv_all.at[slot], slot, on_send.at[i if groups > 4 else i % 2, step], to_plane).start()

    at_end = (below == 0) | (above == 0)

    def send_queries():
        for step in far_first[:-1]:
            q_copy(step).start()

    @pl.when(at_end)
    def _():
        send_queries()

    if groups > 1:
        relay(1, (0,))
    if groups > 3:
        relay(3, (0,))
    for step in near_first[1:]:
        plane_relay(step)
    @pl.when(jnp.logical_not(at_end))
    def _():
        send_queries()

    def late_ways(act):
        both_ways(kv_out.at[member], sp, 0, act, late=True)
        for step in near_first[1:]:
            both_ways(kv_all.at[first + peer(step)], first + peer(step), step, act, late=True)

    late_ways(start)
    if groups > 1 and members > 1:
        relay(1, near_first[1:])
    if groups > 2:
        relay(2, (0,))

    def prepare(slots, offset):
        for c, slot in enumerate(slots):
            flipped = kv_all[slot].astype(f32).T
            vt[ONES:, offset + c * rows:offset + (c + 1) * rows] = flipped[head_dim:].astype(bf)

    pairs = heads // 2
    half = 2 * rows

    def score(slots, place, bank):
        k = jnp.concatenate([kv_all[slot] for slot in slots], axis=0)
        sc[bank, :len(slots) * rows, :place.stop - place.start] = lax.dot_general(
            k, qs[place, :], (((1,), (1,)), ((), ())), preferred_element_type=f32)

    def weigh(count, place, bank, fresh):
        size = place.stop - place.start
        s = sc[bank, :count, :size]
        top = jnp.max(jnp.max(s.reshape(count // 8, 8, size), axis=0), axis=0, keepdims=True)
        now = jnp.broadcast_to(top, (8, size))
        fade = None
        if not fresh:
            before = peak[:, place]
            now = jnp.maximum(before, now)
            fade = jnp.exp(before - now)
        peak[:, place] = now
        pb[bank, :count, :size] = jnp.exp(s - jnp.broadcast_to(now[:1], (count, size))).astype(bf)
        return fade

    def gather(offset, count, place, bank, fade):
        size = place.stop - place.start
        new = jnp.dot(vt[:, offset:offset + count], pb[bank, :count, :size], preferred_element_type=f32)
        if fade is not None:
            new = acc[:, place] * jnp.broadcast_to(fade[:1], (ONES + head_dim, size)) + new
        acc[:, place] = new

    def block(step):
        return slice(step * tall, (step + 1) * tall)

    def run(tasks, fresh=False):
        score(tasks[0][0], tasks[0][2], 0)
        fades, ready = [], []
        for n in range(len(tasks) + 1):
            if n + 1 < len(tasks):
                score(tasks[n + 1][0], tasks[n + 1][2], (n + 1) % 2)
            for step, pair in ready:
                if step:
                    m_copy(step, pair).start()
            ready = []
            if n < len(tasks):
                fades.append(weigh(len(tasks[n][0]) * rows, tasks[n][2], n % 2, fresh))
            if n:
                slots, offset, place, ready = tasks[n - 1]
                gather(offset, len(slots) * rows, place, (n - 1) % 2, fades[n - 1])
                for step, pair in ready:
                    finish(step, pair)
        for step, pair in ready:
            if step:
                m_copy(step, pair).start()

    def m_copy(step, pair):
        at = (step - 1) * pairs + pair
        return sp_copy(m_out.at[step, pair], m_all.at[step, pair], load_sem.at[1 + at], m_recv.at[at], first + peer(step))

    def finish(step, pair):
        halves = []
        for g in (2 * pair, 2 * pair + 1):
            piece = acc[:, (step * heads + g) * rows:(step * heads + g + 1) * rows]
            halves.append(piece[ONES:] * jnp.concatenate([1.0 / piece[:8]] * (head_dim // 8), axis=0))
        (m_out if step else m_all)[step, pair] = jnp.concatenate(halves, axis=0).T.astype(bf)

    def slots_of(i):
        base, _, needed = onward(i)
        return [base + peer(step) for step in near_first], needed

    def fetch(slots, needed):
        @pl.when(jnp.logical_not(needed))
        def _():
            for slot in slots:
                wait_kv(slot)

    own = [sp if step == 0 else first + peer(step) for step in near_first]
    spread(0, q_out[0])
    prepare(own, 0)
    run([(own, 0, block(0), ())], fresh=True)
    if groups > 2 and members > 1:
        relay(2, near_first[1:])
    if groups > 3 and members > 1:
        relay(3, near_first[1:])
    for step in range(1, members):
        sp_copy(q_out.at[step], q_all.at[step], load_sem.at[peers + step], q_recv.at[step - 1], first + peer(step)).wait_recv()
        spread(step, q_all[step])
    if members > 1:
        run([(own, 0, block(step), ()) for step in near_first[1:]], fresh=True)

    deferred = groups == 4 and members > 1
    spare = 2 * keys

    def whole_group(i, carry):
        slots, needed = slots_of(i)
        fetch(slots, needed)
        prepare(slots, spare)
        run([(slots, spare, block(step), ()) for step in near_first[1 if deferred else 0:]])
        if groups > 4:
            @pl.when(i + 3 < groups)
            def _():
                relay(i + 3, near_first)
        return carry

    if groups > 1:
        joined = max(1, groups - 2)
        if deferred:
            whole_group(1, 0)
        else:
            lax.fori_loop(1, joined, whole_group, 0)
        last_slots = []
        for i in range(joined, groups):
            slots, needed = slots_of(i)
            fetch(slots, needed)
            prepare(slots, len(last_slots) * rows)
            last_slots += slots
        every = tuple(range(pairs))
        tasks = []
        for step in far_first[:-1]:
            if HALVES:
                tasks += [(last_slots, 0, slice(step * tall + pair * half, step * tall + (pair + 1) * half), ((step, pair),))
                          for pair in every]
            else:
                tasks.append((last_slots, 0, block(step), tuple((step, pair) for pair in every)))
        if deferred:
            tasks.append((slots_of(1)[0], spare, block(0), ()))
        tasks.append((last_slots, 0, block(0), tuple((0, pair) for pair in every)))
        for step in near_first[1:]:
            kv_copy(step).wait_send()
            q_copy(step).wait_send()
        run(tasks)
    else:
        for step in near_first[1:]:
            kv_copy(step).wait_send()
            q_copy(step).wait_send()
        for step in far_first:
            for pair in range(pairs):
                finish(step, pair)
                if step:
                    m_copy(step, pair).start()

    loads[small + 5].wait()
    cut_out = wo.shape[1] // O_CUTS

    def o_copy(step, j):
        cols = pl.ds(j * cut_out, cut_out)
        return tp_copy(o_out.at[step, :, cols], o_in.at[step, :, cols], load_sem.at[1 + peers * max(2, width // LANES) + (step - 1) * O_CUTS + j], o_recv.at[step - 1, j],
                       (tp + step) % n_tp)

    def mixed_share(step, j):
        share = pl.ds(pl.multiple_of(peer(step) * width, width), width)
        mixed = jnp.concatenate([m_all[step, pair] for pair in range(pairs)], axis=1)
        return jnp.dot(mixed, wo[share, j * cut_out:(j + 1) * cut_out], preferred_element_type=f32)

    for step in (0, *far_first[:-1]):
        if step:
            for pair in range(pairs):
                m_copy(step, pair).wait_recv()
        term = mixed_share(step, 0)
        for j in range(O_CUTS):
            cols = slice(j * cut_out, (j + 1) * cut_out)
            total = o_acc[:, cols] + term if step else term
            if j + 1 < O_CUTS:
                term = mixed_share(step, j + 1)
            o_acc[:, cols] = total
            if step == min(1, members - 1):
                for other in range(1, n_tp):
                    o_out[other, :, cols] = o_acc[own_slice((tp + other) % n_tp), cols].astype(bf)
                    o_copy(other, j).start()
    for j in range(O_CUTS):
        cols = slice(j * cut_out, (j + 1) * cut_out)
        result = o_acc[own_slice(tp), cols].astype(bf).astype(f32)
        for other in range(1, n_tp):
            o_copy(other, j).wait_recv()
            result = result + o_in[other, :, cols].astype(f32)
        out_ref[:, cols] = result.astype(bf)

    for j in range(X_CUTS):
        for step in range(1, n_tp):
            x_copy(step, j).wait_send()
    for j in range(O_CUTS):
        for step in range(1, n_tp):
            o_copy(step, j).wait_send()
    both_ways(kv_out.at[member], sp, 0, wait_send)
    late_ways(wait_send)
    for step in range(1, members):
        for pair in range(pairs):
            m_copy(step, pair).wait_send()
        both_ways(kv_all.at[first + peer(step)], first + peer(step), step, wait_send)
        if step in crossing:
            straight(step, wait_send)

    def sent(i, carry):
        base, to_plane, needed = onward(i)

        @pl.when(needed)
        def _():
            for step in near_first:
                slot = base + peer(step)
                line(kv_all.at[slot], slot, on_send.at[i if groups > 4 else i % 2, step], to_plane).wait_send()

        return carry

    lax.fori_loop(1, groups, sent, 0)


def solution(mesh):
    n_sp, n_tp = mesh.shape["sp"], mesh.shape["tp"]

    def body(tokens_in, w_query, w_key, w_value, w_out, q_gain, k_gain):
        head_dim = q_gain.shape[0]
        own_rows, depth = tokens_in.shape
        rows = own_rows * n_tp
        query_cols, key_cols = w_query.shape[1], w_key.shape[1]
        members = key_cols // head_dim
        width = query_cols // members
        heads = width // head_dim
        if key_cols % LANES:
            wkv = (jnp.concatenate([w_key, w_value], axis=1),)
        else:
            wkv = (w_key, w_value)
        row_table, col_table = tables(rows * n_sp, head_dim)
        bf, f32 = jnp.bfloat16, jnp.float32
        hbm = pl.BlockSpec(memory_space=pltpu.HBM)
        vmem = pl.BlockSpec(memory_space=pltpu.VMEM)
        dma = pltpu.SemaphoreType.DMA
        out_cols = w_out.shape[1]
        groups, peers = n_sp // members, max(1, members - 1)
        call = pl.pallas_call(
            functools.partial(kernel, n_sp, n_tp, members, head_dim),
            out_shape=pltpu.VMEM((own_rows, out_cols), bf),
            in_specs=[hbm, hbm, (hbm,) * len(wkv), hbm, hbm, hbm, hbm, hbm],
            out_specs=vmem,
            scratch_shapes=[
                pltpu.VMEM((rows, depth), bf),
                pltpu.VMEM(w_query.shape, bf),
                tuple(pltpu.VMEM(w.shape, bf) for w in wkv),
                pltpu.VMEM(w_out.shape, bf),
                pltpu.VMEM(row_table.shape, f32),
                pltpu.VMEM(col_table.shape, f32),
                pltpu.VMEM((1, head_dim), f32),
                pltpu.VMEM((1, head_dim), f32),
                pltpu.VMEM((members, rows, LANES), bf),
                pltpu.VMEM((n_sp, rows, LANES), bf),
                pltpu.VMEM((members, rows, width), bf),
                pltpu.VMEM((members, rows, width), bf),
                pltpu.VMEM((members * heads * rows, LANES), bf),
                pltpu.VMEM((ONES + head_dim, 3 * members * rows), bf),
                pltpu.VMEM((2, 2 * members * rows, heads * rows), f32),
                pltpu.VMEM((2, 2 * members * rows, heads * rows), bf),
                pltpu.VMEM((ONES + head_dim, members * heads * rows), f32),
                pltpu.VMEM((8, members * heads * rows), f32),
                pltpu.VMEM((members, width // LANES, rows, LANES), bf),
                pltpu.VMEM((members, width // LANES, rows, LANES), bf),
                pltpu.VMEM((rows, out_cols), f32),
                pltpu.VMEM((n_tp, own_rows, out_cols), bf),
                pltpu.VMEM((n_tp, own_rows, out_cols), bf),
                dma((max(7 + len(wkv), 1 + peers * max(2, width // LANES) + (n_tp - 1) * O_CUTS),)),
                dma((n_tp - 1, X_CUTS)), dma((n_tp - 1, X_CUTS)),
                dma((n_sp,)), dma((3 if groups <= 4 else 4, members)),
                dma((2 if groups <= 4 else groups, members)),
                dma((peers,)), dma((peers * (width // LANES),)),
                dma((n_tp - 1, O_CUTS)),
            ],
            compiler_params=pltpu.CompilerParams(
                collective_id=0, has_side_effects=True, vmem_limit_bytes=56 * 1024 * 1024),
        )
        return call(tokens_in, w_query, wkv, w_out, jnp.asarray(row_table), jnp.asarray(col_table),
                    q_gain.reshape(1, head_dim), k_gain.reshape(1, head_dim))

    return jax.shard_map(
        body,
        mesh=mesh,
        in_specs=(
            P(("sp", "tp"), None),
            P(None, "tp"),
            P(None, "tp"),
            P(None, "tp"),
            P("tp", None),
            P(),
            P(),
        ),
        out_specs=P(("sp", "tp"), None),
        check_vma=False,
    )
```

```python
import functools

import jax
import jax.numpy as jnp
import numpy as np
from jax import lax
from jax.experimental import pallas as pl
from jax.experimental.pallas import tpu as pltpu
from jax.sharding import PartitionSpec as P

GRID_W = 64
LANES = 128
ONES = 16
X_CUTS = 1
O_CUTS = 1
STRAIGHT = (1, 2)
HALVES = False
LATE_BESIDE = False


def tables(token_count, head_dim):
    pairs = head_dim // 4
    lane = np.arange(LANES)
    freq = 10000.0 ** (-(lane % pairs) / pairs)
    sign = np.where(lane % (2 * pairs) < pairs, -1.0, 1.0)

    def both(count):
        angle = np.arange(count)[:, None] * freq[None, :]
        return np.concatenate([np.cos(angle), np.sin(angle) * sign], axis=1).astype(np.float32)

    return both(token_count // GRID_W), both(GRID_W)


def kernel(
    n_sp, n_tp, members, head_dim,
    tok_hbm, wq_hbm, wkv_hbms, wo_hbm, row_hbm, col_hbm, qg_hbm, kg_hbm, out_ref,
    x, wq, wkvs, wo, row_ref, col_ref, qg_ref, kg_ref,
    kv_out, kv_all, q_out, q_all, qs, vt, sc, pb, acc, peak, m_out, m_all, o_acc, o_out, o_in,
    load_sem, x_send, x_recv, kv_recv, own_send, on_send, q_recv, m_recv, o_recv,
):
    bf, f32 = jnp.bfloat16, jnp.float32
    sp, tp = lax.axis_index("sp"), lax.axis_index("tp")
    own_rows, depth = tok_hbm.shape
    rows = own_rows * n_tp
    groups = n_sp // members
    plane, member = sp // members, sp % members
    width = wq.shape[1] // members
    heads = width // head_dim
    tall = heads * rows
    keys = members * rows
    first = plane * members
    below, above = plane, groups - 1 - plane
    peers = max(1, members - 1)
    both_sides = jnp.minimum(below, above)

    def peer(step):
        other, bit = member, 1
        while bit <= step:
            if step & bit:
                other = other + bit - 2 * bit * ((member // bit) % 2)
            bit *= 2
        return other

    def sp_copy(src, dst, send, recv, to):
        return pltpu.make_async_remote_copy(
            src_ref=src, dst_ref=dst, send_sem=send, recv_sem=recv,
            device_id={"sp": to}, device_id_type=pl.DeviceIdType.MESH)

    def tp_copy(src, dst, send, recv, to):
        return pltpu.make_async_remote_copy(
            src_ref=src, dst_ref=dst, send_sem=send, recv_sem=recv,
            device_id={"tp": to}, device_id_type=pl.DeviceIdType.MESH)

    def own_slice(index):
        return pl.ds(pl.multiple_of(index * own_rows, own_rows), own_rows)

    def way(i):
        paired = i <= 2 * both_sides
        distance = jnp.where(paired, (i + 1) // 2, i - both_sides)
        upward = jnp.where(paired, i % 2, jnp.where(above > below, 1, 0))
        return distance, 2 * upward - 1

    barrier = pltpu.get_barrier_semaphore()
    for step in range(1, n_tp):
        pl.semaphore_signal(barrier, inc=1, device_id={"tp": (tp + step) % n_tp}, device_id_type=pl.DeviceIdType.MESH)
    for step in range(1, members):
        pl.semaphore_signal(barrier, inc=1, device_id={"sp": first + peer(step)}, device_id_type=pl.DeviceIdType.MESH)

    def greet(when, to):
        @pl.when(when)
        def _():
            pl.semaphore_signal(barrier, inc=1, device_id={"sp": to}, device_id_type=pl.DeviceIdType.MESH)

    crossing = [step for step in STRAIGHT if step < members]
    greet(below > 0, sp - members)
    greet(above > 0, sp + members)
    greet((below > 1) & (above > 0), sp - 2 * members)
    greet((above > 1) & (below > 0), sp + 2 * members)
    for step in crossing:
        greet((plane < 2) & (above > 0), (plane + 1) * members + peer(step))
        greet((plane > 1) & (above > 1), (plane + 2) * members + peer(step))
        greet((plane == 0) & (above > 2), (plane + 3) * members + peer(step))
    greet((plane == 0) & (above > 2), sp + 3 * members)

    def count(fact):
        return jnp.where(fact, 1, 0)

    targets = (n_tp - 1 + members - 1 + count(below > 0) + count(above > 0) + count(below > 2) + count(above > 2) + count(below == 3)
               + len(crossing) * count(below > 0))

    small = 1 + len(wkvs)
    pairs_of = [(tok_hbm, x.at[own_slice(tp)]), *zip(wkv_hbms, wkvs), (row_hbm, row_ref), (col_hbm, col_ref),
                (qg_hbm, qg_ref), (kg_hbm, kg_ref), (wq_hbm, wq), (wo_hbm, wo)]
    loads = [pltpu.make_async_copy(src, dst, load_sem.at[(i + 1) % len(pairs_of)]) for i, (src, dst) in enumerate(pairs_of)]
    for load in loads:
        load.start()

    lane = lax.broadcasted_iota(jnp.int32, (rows, LANES), 1)
    low = lane % head_dim < head_dim // 2
    left = lane % (head_dim // 2) < head_dim // 4
    even = lane < head_dim
    ones_r = lax.broadcasted_iota(jnp.int32, (LANES, LANES), 0) // head_dim
    ones_c = lax.broadcasted_iota(jnp.int32, (LANES, LANES), 1) // head_dim
    block = jnp.where(ones_r == ones_c, 1.0, 0.0).astype(bf)
    vt[:ONES, :] = jnp.ones((ONES, 3 * keys), bf)

    loads[0].wait()
    pl.semaphore_wait(barrier, targets)
    cut_depth = depth // X_CUTS

    def x_copy(step, j):
        cols = pl.ds(j * cut_depth, cut_depth)
        return tp_copy(x.at[own_slice(tp), cols], x.at[own_slice(tp), cols], x_send.at[step - 1, j], x_recv.at[step - 1, j],
                       (tp + step) % n_tp)

    for j in range(X_CUTS):
        for step in range(1, n_tp):
            x_copy(step, j).start()
    for load in loads[small:small + 4]:
        load.wait()
    cos_parts, sin_parts = [], []
    per_dev = rows // GRID_W
    low_g = low[:GRID_W]
    for i in range(per_dev):
        line = row_ref[pl.ds(sp * per_dev + i, 1), :]
        cos_parts.append(jnp.where(low_g, jnp.broadcast_to(line[:, :LANES], (GRID_W, LANES)), col_ref[:, :LANES]))
        sin_parts.append(jnp.where(low_g, jnp.broadcast_to(line[:, LANES:], (GRID_W, LANES)), col_ref[:, LANES:]))
    cosine = jnp.concatenate(cos_parts, axis=0)
    sine = jnp.concatenate(sin_parts, axis=0)
    gain_q = jnp.concatenate([qg_ref[...]] * (LANES // head_dim), axis=1) * head_dim ** (-0.5)
    gain_k = jnp.concatenate([kg_ref[...]] * (LANES // head_dim), axis=1)

    def turned(u, gain):
        square = u * u
        high = square.astype(bf)
        rest = (square - high.astype(f32)).astype(bf)
        total = jnp.dot(high, block, preferred_element_type=f32) + jnp.dot(
            rest, block, preferred_element_type=f32)
        n = u * lax.rsqrt(total * (1.0 / head_dim) + 1e-06) * gain
        quarter = head_dim // 4
        other = jnp.where(left, pltpu.roll(n, LANES - quarter, 1), pltpu.roll(n, quarter, 1))
        return n * cosine + other * sine

    for load in loads[1:small]:
        load.wait()
    sums = [None] * len(wkvs)
    for j in range(X_CUTS):
        cols = slice(j * cut_depth, (j + 1) * cut_depth)
        for step in range(1, n_tp):
            theirs = x.at[own_slice((tp + n_tp - step) % n_tp), pl.ds(j * cut_depth, cut_depth)]
            tp_copy(theirs, theirs, x_send.at[step - 1, j], x_recv.at[step - 1, j], (tp + step) % n_tp).wait_recv()
        for i in range(len(wkvs)):
            part = jnp.dot(x[:, cols], wkvs[i][cols, :], preferred_element_type=f32)
            sums[i] = part if j == 0 else sums[i] + part
    sums = [s.astype(bf).astype(f32) for s in sums]
    if len(wkvs) == 2:
        for pair in range(members // 2):
            cut = slice(pair * LANES, (pair + 1) * LANES)
            k, v = turned(sums[0][:, cut], gain_k), sums[1][:, cut]
            kv_out[2 * pair] = jnp.where(even, k, pltpu.roll(v, head_dim, 1)).astype(bf)
            kv_out[2 * pair + 1] = jnp.where(even, pltpu.roll(k, head_dim, 1), v).astype(bf)
    else:
        kv_out[0] = jnp.where(even, turned(sums[0], gain_k), sums[0]).astype(bf)

    def kv_copy(step):
        return sp_copy(kv_out.at[peer(step)], kv_all.at[sp], load_sem.at[step], kv_recv.at[sp], first + peer(step))

    def line(src, slot, send, to_plane):
        return sp_copy(src, kv_all.at[slot], send, kv_recv.at[slot], to_plane * members + member)

    def both_ways(src, slot, step, act, late=False):
        if step in crossing:
            far, beside, beyond = below < 0, below > 2, below == 3
        else:
            far, beside, beyond = below == 3, below > 0, below > 2
        if late:
            @pl.when(below == 3)
            def _():
                if LATE_BESIDE:
                    act(line(src, slot, own_send.at[0, step], plane - 1))
                act(line(src, slot, own_send.at[own_send.shape[0] - 1 if groups > 4 else 1, step], plane - 2))

            return

        @pl.when(far)
        def _():
            act(line(src, slot, own_send.at[2, step], plane - 3))

        @pl.when(beside & (below != 3) if LATE_BESIDE else beside)
        def _():
            act(line(src, slot, own_send.at[0, step], plane - 1))

        @pl.when(above > 0)
        def _():
            act(line(src, slot, own_send.at[1, step], plane + 1))

        @pl.when(beyond & (below != 3))
        def _():
            act(line(src, slot, own_send.at[own_send.shape[0] - 1 if groups > 4 else 1, step], plane - 2))

        @pl.when(above > 2)
        def _():
            act(line(src, slot, own_send.at[2, step], plane + 2))

    def straight(step, act):
        to_plane = jnp.where(plane > 3, plane - 2, jnp.where(plane == 3, plane - 3, plane - 1))

        @pl.when(plane > 0)
        def _():
            act(sp_copy(kv_out.at[peer(step)], kv_all.at[sp], own_send.at[jnp.where(plane > 3, own_send.shape[0] - 1, jnp.where(plane == 3, 2, 0)), step], kv_recv.at[sp],
                        to_plane * members + peer(step)))

    def start(copy):
        copy.start()

    def wait_send(copy):
        copy.wait_send()

    def wait_kv(slot):
        sp_copy(kv_all.at[slot], kv_all.at[slot], load_sem.at[1], kv_recv.at[slot], sp).wait_recv()

    both_ways(kv_out.at[member], sp, 0, start)
    for step in range(1, members):
        kv_copy(step).start()
    for step in crossing:
        straight(step, start)
    kv_all[sp] = kv_out[member]

    loads[small + 4].wait()

    def q_copy(step):
        return sp_copy(q_out.at[step], q_all.at[step], load_sem.at[peers + step], q_recv.at[step - 1], first + peer(step))

    def spread(step, q):
        for g in range(heads):
            u = q[:, (g // 2) * LANES:(g // 2 + 1) * LANES].astype(f32)
            u = u if g % 2 == 0 else pltpu.roll(u, head_dim, 1)
            qs[(step * heads + g) * rows:(step * heads + g + 1) * rows, :] = jnp.where(even, u, 0.0).astype(bf)

    def plane_relay(step):
        slot = first + peer(step)
        wait_kv(slot)
        both_ways(kv_all.at[slot], slot, step, start)

    def raw_queries(step):
        part = wq[:, pl.ds(pl.multiple_of(peer(step) * width, width), width)]
        return jnp.dot(x[...], part, preferred_element_type=f32)

    order = (*range(members - 1, 0, -1), 0)
    raw = raw_queries(order[0])
    for n, step in enumerate(order):
        u = raw.astype(bf).astype(f32)
        if n + 1 < members:
            raw = raw_queries(order[n + 1])
        for t in range(width // LANES):
            cut = slice(t * LANES, (t + 1) * LANES)
            q_out[step, :, cut] = turned(u[:, cut], gain_q).astype(bf)
    near_first = tuple(range(members))
    far_first = (*range(members - 1, 0, -1), 0)

    def onward(i):
        distance, side = way(i)
        target = plane - side
        inside = (target > 0) & (target < groups - 1)
        beyond = (distance > 1) & jnp.logical_not((distance == 2) & (target == 0) & (side > 0))
        needed = (target >= 0) & (target < groups) & (beyond | ((distance == 1) & jnp.logical_not(inside)))
        return (plane + distance * side) * members, target, needed

    def relay(i, steps):
        base, to_plane, needed = onward(i)

        @pl.when(needed)
        def _():
            for step in steps:
                slot = base + peer(step)
                wait_kv(slot)
                line(kv_all.at[slot], slot, on_send.at[i if groups > 4 else i % 2, step], to_plane).start()

    at_end = (below == 0) | (above == 0)

    def send_queries():
        for step in far_first[:-1]:
            q_copy(step).start()

    @pl.when(at_end)
    def _():
        send_queries()

    if groups > 1:
        relay(1, (0,))
    if groups > 3:
        relay(3, (0,))
    for step in near_first[1:]:
        plane_relay(step)
    @pl.when(jnp.logical_not(at_end))
    def _():
        send_queries()

    def late_ways(act):
        both_ways(kv_out.at[member], sp, 0, act, late=True)
        for step in near_first[1:]:
            both_ways(kv_all.at[first + peer(step)], first + peer(step), step, act, late=True)

    late_ways(start)
    if groups > 1 and members > 1:
        relay(1, near_first[1:])
    if groups > 2:
        relay(2, (0,))

    def prepare(slots, offset):
        for c, slot in enumerate(slots):
            flipped = kv_all[slot].astype(f32).T
            vt[ONES:, offset + c * rows:offset + (c + 1) * rows] = flipped[head_dim:].astype(bf)

    pairs = heads // 2
    half = 2 * rows

    def score(slots, place, bank):
        k = jnp.concatenate([kv_all[slot] for slot in slots], axis=0)
        sc[bank, :len(slots) * rows, :place.stop - place.start] = lax.dot_general(
            k, qs[place, :], (((1,), (1,)), ((), ())), preferred_element_type=f32)

    def weigh(count, place, bank, fresh):
        size = place.stop - place.start
        s = sc[bank, :count, :size]
        top = jnp.max(jnp.max(s.reshape(count // 8, 8, size), axis=0), axis=0, keepdims=True)
        now = jnp.broadcast_to(top, (8, size))
        fade = None
        if not fresh:
            before = peak[:, place]
            now = jnp.maximum(before, now)
            fade = jnp.exp(before - now)
        peak[:, place] = now
        pb[bank, :count, :size] = jnp.exp(s - jnp.broadcast_to(now[:1], (count, size))).astype(bf)
        return fade

    def gather(offset, count, place, bank, fade):
        size = place.stop - place.start
        new = jnp.dot(vt[:, offset:offset + count], pb[bank, :count, :size], preferred_element_type=f32)
        if fade is not None:
            new = acc[:, place] * jnp.broadcast_to(fade[:1], (ONES + head_dim, size)) + new
        acc[:, place] = new

    def block(step):
        return slice(step * tall, (step + 1) * tall)

    def run(tasks, fresh=False):
        score(tasks[0][0], tasks[0][2], 0)
        fades, ready = [], []
        for n in range(len(tasks) + 1):
            if n + 1 < len(tasks):
                score(tasks[n + 1][0], tasks[n + 1][2], (n + 1) % 2)
            for step, pair in ready:
                if step:
                    m_copy(step, pair).start()
            ready = []
            if n < len(tasks):
                fades.append(weigh(len(tasks[n][0]) * rows, tasks[n][2], n % 2, fresh))
            if n:
                slots, offset, place, ready = tasks[n - 1]
                gather(offset, len(slots) * rows, place, (n - 1) % 2, fades[n - 1])
                for step, pair in ready:
                    finish(step, pair)
        for step, pair in ready:
            if step:
                m_copy(step, pair).start()

    def m_copy(step, pair):
        at = (step - 1) * pairs + pair
        return sp_copy(m_out.at[step, pair], m_all.at[step, pair], load_sem.at[1 + at], m_recv.at[at], first + peer(step))

    def finish(step, pair):
        halves = []
        for g in (2 * pair, 2 * pair + 1):
            piece = acc[:, (step * heads + g) * rows:(step * heads + g + 1) * rows]
            halves.append(piece[ONES:] * jnp.concatenate([1.0 / piece[:8]] * (head_dim // 8), axis=0))
        (m_out if step else m_all)[step, pair] = jnp.concatenate(halves, axis=0).T.astype(bf)

    def slots_of(i):
        base, _, needed = onward(i)
        return [base + peer(step) for step in near_first], needed

    def fetch(slots, needed):
        @pl.when(jnp.logical_not(needed))
        def _():
            for slot in slots:
                wait_kv(slot)

    own = [sp if step == 0 else first + peer(step) for step in near_first]
    spread(0, q_out[0])
    prepare(own, 0)
    run([(own, 0, block(0), ())], fresh=True)
    if groups > 2 and members > 1:
        relay(2, near_first[1:])
    if groups > 3 and members > 1:
        relay(3, near_first[1:])
    for step in range(1, members):
        sp_copy(q_out.at[step], q_all.at[step], load_sem.at[peers + step], q_recv.at[step - 1], first + peer(step)).wait_recv()
        spread(step, q_all[step])
    if members > 1:
        run([(own, 0, block(step), ()) for step in near_first[1:]], fresh=True)

    deferred = groups == 4 and members > 1
    spare = 2 * keys

    def whole_group(i, carry):
        slots, needed = slots_of(i)
        fetch(slots, needed)
        prepare(slots, spare)
        run([(slots, spare, block(step), ()) for step in near_first[1 if deferred else 0:]])
        if groups > 4:
            @pl.when(i + 3 < groups)
            def _():
                relay(i + 3, near_first)
        return carry

    if groups > 1:
        joined = max(1, groups - 2)
        if deferred:
            whole_group(1, 0)
        else:
            lax.fori_loop(1, joined, whole_group, 0)
        last_slots = []
        for i in range(joined, groups):
            slots, needed = slots_of(i)
            fetch(slots, needed)
            prepare(slots, len(last_slots) * rows)
            last_slots += slots
        every = tuple(range(pairs))
        tasks = []
        for step in far_first[:-1]:
            if HALVES:
                tasks += [(last_slots, 0, slice(step * tall + pair * half, step * tall + (pair + 1) * half), ((step, pair),))
                          for pair in every]
            else:
                tasks.append((last_slots, 0, block(step), tuple((step, pair) for pair in every)))
        if deferred:
            tasks.append((slots_of(1)[0], spare, block(0), ()))
        tasks.append((last_slots, 0, block(0), tuple((0, pair) for pair in every)))
        for step in near_first[1:]:
            kv_copy(step).wait_send()
            q_copy(step).wait_send()
        run(tasks)
    else:
        for step in near_first[1:]:
            kv_copy(step).wait_send()
            q_copy(step).wait_send()
        for step in far_first:
            for pair in range(pairs):
                finish(step, pair)
                if step:
                    m_copy(step, pair).start()

    loads[small + 5].wait()
    cut_out = wo.shape[1] // O_CUTS

    def o_copy(step, j):
        cols = pl.ds(j * cut_out, cut_out)
        return tp_copy(o_out.at[step, :, cols], o_in.at[step, :, cols], load_sem.at[1 + peers * max(2, width // LANES) + (step - 1) * O_CUTS + j], o_recv.at[step - 1, j],
                       (tp + step) % n_tp)

    def mixed_share(step, j):
        share = pl.ds(pl.multiple_of(peer(step) * width, width), width)
        mixed = jnp.concatenate([m_all[step, pair] for pair in range(pairs)], axis=1)
        return jnp.dot(mixed, wo[share, j * cut_out:(j + 1) * cut_out], preferred_element_type=f32)

    for step in (0, *far_first[:-1]):
        if step:
            for pair in range(pairs):
                m_copy(step, pair).wait_recv()
        term = mixed_share(step, 0)
        for j in range(O_CUTS):
            cols = slice(j * cut_out, (j + 1) * cut_out)
            total = o_acc[:, cols] + term if step else term
            if j + 1 < O_CUTS:
                term = mixed_share(step, j + 1)
            o_acc[:, cols] = total
            if step == min(1, members - 1):
                for other in range(1, n_tp):
                    o_out[other, :, cols] = o_acc[own_slice((tp + other) % n_tp), cols].astype(bf)
                    o_copy(other, j).start()
    for j in range(O_CUTS):
        cols = slice(j * cut_out, (j + 1) * cut_out)
        result = o_acc[own_slice(tp), cols].astype(bf).astype(f32)
        for other in range(1, n_tp):
            o_copy(other, j).wait_recv()
            result = result + o_in[other, :, cols].astype(f32)
        out_ref[:, cols] = result.astype(bf)

    for j in range(X_CUTS):
        for step in range(1, n_tp):
            x_copy(step, j).wait_send()
    for j in range(O_CUTS):
        for step in range(1, n_tp):
            o_copy(step, j).wait_send()
    both_ways(kv_out.at[member], sp, 0, wait_send)
    late_ways(wait_send)
    for step in range(1, members):
        for pair in range(pairs):
            m_copy(step, pair).wait_send()
        both_ways(kv_all.at[first + peer(step)], first + peer(step), step, wait_send)
        if step in crossing:
            straight(step, wait_send)

    def sent(i, carry):
        base, to_plane, needed = onward(i)

        @pl.when(needed)
        def _():
            for step in near_first:
                slot = base + peer(step)
                line(kv_all.at[slot], slot, on_send.at[i if groups > 4 else i % 2, step], to_plane).wait_send()

        return carry

    lax.fori_loop(1, groups, sent, 0)


def solution(mesh):
    n_sp, n_tp = mesh.shape["sp"], mesh.shape["tp"]

    def body(tokens_in, w_query, w_key, w_value, w_out, q_gain, k_gain):
        head_dim = q_gain.shape[0]
        own_rows, depth = tokens_in.shape
        rows = own_rows * n_tp
        query_cols, key_cols = w_query.shape[1], w_key.shape[1]
        members = key_cols // head_dim
        width = query_cols // members
        heads = width // head_dim
        if key_cols % LANES:
            wkv = (jnp.concatenate([w_key, w_value], axis=1),)
        else:
            wkv = (w_key, w_value)
        row_table, col_table = tables(rows * n_sp, head_dim)
        bf, f32 = jnp.bfloat16, jnp.float32
        hbm = pl.BlockSpec(memory_space=pltpu.HBM)
        vmem = pl.BlockSpec(memory_space=pltpu.VMEM)
        dma = pltpu.SemaphoreType.DMA
        out_cols = w_out.shape[1]
        groups, peers = n_sp // members, max(1, members - 1)
        call = pl.pallas_call(
            functools.partial(kernel, n_sp, n_tp, members, head_dim),
            out_shape=pltpu.VMEM((own_rows, out_cols), bf),
            in_specs=[hbm, hbm, (hbm,) * len(wkv), hbm, hbm, hbm, hbm, hbm],
            out_specs=vmem,
            scratch_shapes=[
                pltpu.VMEM((rows, depth), bf),
                pltpu.VMEM(w_query.shape, bf),
                tuple(pltpu.VMEM(w.shape, bf) for w in wkv),
                pltpu.VMEM(w_out.shape, bf),
                pltpu.VMEM(row_table.shape, f32),
                pltpu.VMEM(col_table.shape, f32),
                pltpu.VMEM((1, head_dim), f32),
                pltpu.VMEM((1, head_dim), f32),
                pltpu.VMEM((members, rows, LANES), bf),
                pltpu.VMEM((n_sp, rows, LANES), bf),
                pltpu.VMEM((members, rows, width), bf),
                pltpu.VMEM((members, rows, width), bf),
                pltpu.VMEM((members * heads * rows, LANES), bf),
                pltpu.VMEM((ONES + head_dim, 3 * members * rows), bf),
                pltpu.VMEM((2, 2 * members * rows, heads * rows), f32),
                pltpu.VMEM((2, 2 * members * rows, heads * rows), bf),
                pltpu.VMEM((ONES + head_dim, members * heads * rows), f32),
                pltpu.VMEM((8, members * heads * rows), f32),
                pltpu.VMEM((members, width // LANES, rows, LANES), bf),
                pltpu.VMEM((members, width // LANES, rows, LANES), bf),
                pltpu.VMEM((rows, out_cols), f32),
                pltpu.VMEM((n_tp, own_rows, out_cols), bf),
                pltpu.VMEM((n_tp, own_rows, out_cols), bf),
                dma((max(7 + len(wkv), 1 + peers * max(2, width // LANES) + (n_tp - 1) * O_CUTS),)),
                dma((n_tp - 1, X_CUTS)), dma((n_tp - 1, X_CUTS)),
                dma((n_sp,)), dma((3 if groups <= 4 else 4, members)),
                dma((2 if groups <= 4 else groups, members)),
                dma((peers,)), dma((peers * (width // LANES),)),
                dma((n_tp - 1, O_CUTS)),
            ],
            compiler_params=pltpu.CompilerParams(
                collective_id=0, has_side_effects=True, vmem_limit_bytes=56 * 1024 * 1024),
        )
        return call(tokens_in, w_query, wkv, w_out, jnp.asarray(row_table), jnp.asarray(col_table),
                    q_gain.reshape(1, head_dim), k_gain.reshape(1, head_dim))

    return jax.shard_map(
        body,
        mesh=mesh,
        in_specs=(
            P(("sp", "tp"), None),
            P(None, "tp"),
            P(None, "tp"),
            P(None, "tp"),
            P("tp", None),
            P(),
            P(),
        ),
        out_specs=P(("sp", "tp"), None),
        check_vma=False,
    )
```
